256 devices in a mesh: sp: 64 (over z, x, core), tp: 4 (over y).
Axes of the slice: x: 4, y: 4, z: 8, core: 2. Of those that a mesh axis runs over, the one named last changes fastest.
Arguments:
- queries: bfloat16 [12288, 1536], P('sp', 'tp'), may hold values from -64 to 64
- latents: bfloat16 [12288, 512], P('sp'), may hold values from -6 to 6
- rope_key: bfloat16 [12288, 32], P('sp'), may hold values from -64 to 64
- w_key: bfloat16 [512, 1024], P(None, 'tp'), may hold values from -0.25 to 0.25
- w_value: bfloat16 [512, 1024], P(None, 'tp'), may hold values from -0.25 to 0.25
- w_out: bfloat16 [1024, 2048], P('tp'), may hold values from -0.59765625 to 0.59765625
- resid: bfloat16 [12288, 2048], P('sp', 'tp'), may hold values from -12 to 12
- gain_mix: float32 [2048], P('tp'), may hold values from 0.1 to 1.9
- w_gate: bfloat16 [2048, 3072], P('sp', 'tp'), may hold values from -0.125 to 0.125
- w_up: bfloat16 [2048, 3072], P('sp', 'tp'), may hold values from -0.125 to 0.125
- w_down: bfloat16 [3072, 2048], P('tp', 'sp'), may hold values from -0.41992188 to 0.41992188
- gain_out: float32 [2048], P('tp'), may hold values from 0.1 to 1.9
Outputs:
- layer_out: bfloat16 [12288, 2048], P('sp', 'tp')
The draws below stay inside these ranges and needn't reach their ends.
All inputs are finite; a program needn't handle non-finite values.
Results may differ from the reference program's by a relative error of at most 0.014.
Values may be sent and summed in bfloat16 or wider, within the bound.
A program may use at most 128 MiB of HBM per device.

```python
import math
import jax
import jax.numpy as jnp
from jax import lax

D = 2048
HEADS = 16
NOPE = 64
ROPE = 32
VDIM = 64
KV_RANK = 512
FF = 3072
GRID_W = 64
TOKENS = 12288
N_TP = 4


def drawn_pair(key):
    query_seed = jax.random.fold_in(key, 11)
    rotary_seed = jax.random.fold_in(key, 12)
    width_total = HEADS * (NOPE + ROPE)
    queries = jnp.clip(jax.random.normal(query_seed, (TOKENS, width_total), jnp.float32) * 2.5, -15.0, 15.0)
    rotary = jnp.clip(jax.random.normal(rotary_seed, (TOKENS, ROPE), jnp.float32), -6.0, 6.0)
    return (queries, rotary)


def draw_queries(key, part):
    return drawn_pair(key)[0].astype(jnp.bfloat16)


def draw_rope_key(key, part):
    return drawn_pair(key)[1].astype(jnp.bfloat16)


def draw_resid(key, part):
    row_seed = jax.random.fold_in(key, 21)
    value_seed = jax.random.fold_in(key, 22)
    column_scale = 0.6 * 10.0 ** (jnp.arange(D, dtype=jnp.float32) / (D - 1) - 0.5)
    row_scale = 10.0 ** jax.random.uniform(row_seed, (TOKENS, 1), jnp.float32, -0.5, 0.5)
    values_out = jax.random.normal(value_seed, (TOKENS, D), jnp.float32) * row_scale * column_scale
    return jnp.clip(values_out, -12.0, 12.0).astype(jnp.bfloat16)


def steps_of(key, shape, cuts, low, largest):
    gain, own = 1.0, jax.random.fold_in(key, 6)
    for axis_at, shards_of in cuts:
        draws = jnp.exp(jax.random.uniform(jax.random.fold_in(own, axis_at), (shards_of,), jnp.float32, low / len(cuts), largest / len(cuts)))
        gain = gain * jnp.repeat(draws, shape[axis_at] // shards_of).reshape([-1 if axis == axis_at else 1 for axis in range(len(shape))])
    return gain


def gaussian(stream_key, shape, spread, limit, pieces=(), kind=jnp.bfloat16):
    result = jax.random.normal(stream_key, shape, jnp.float32) * spread
    if len(pieces) > 0:
        result = steps_of(stream_key, shape, pieces, -0.22, 0.18) * result
    return jnp.clip(result, min=-limit, max=limit).astype(kind)


def setup_inputs(seed: int = 0) -> dict:
    keys = jax.random.split(jax.random.key(seed), 13)
    queries = draw_queries(jax.random.fold_in(keys[12], 71), 0)
    latents = gaussian(keys[1], (TOKENS, KV_RANK), 1.0, 6.0, ((0, 64),))
    rope_key = draw_rope_key(jax.random.fold_in(keys[12], 71), 0)
    w_key = gaussian(keys[3], (KV_RANK, HEADS * NOPE), KV_RANK ** -0.5, 0.25, ((1, 4),))
    w_value = gaussian(keys[4], (KV_RANK, HEADS * VDIM), KV_RANK ** -0.5, 0.25, ((1, 4),))
    w_out = gaussian(keys[5], (HEADS * VDIM, D), 0.1, 0.59765625, ((0, 4),))
    resid = draw_resid(jax.random.fold_in(keys[12], 71), 0)
    gain_mix = jnp.clip(1.0 + 0.18 * jax.random.normal(keys[7], (D,), jnp.float32), 0.1, 1.9)
    w_gate = gaussian(keys[8], (D, FF), D ** -0.5, 0.125, ((0, 64), (1, 4)))
    w_up = gaussian(keys[9], (D, FF), D ** -0.5, 0.125, ((0, 64), (1, 4)))
    w_down = gaussian(keys[10], (FF, D), 0.07, 0.41992188, ((0, 4), (1, 64)))
    gain_out = jnp.clip(1.0 + 0.18 * jax.random.normal(keys[11], (D,), jnp.float32), 0.1, 1.9)
    return {"queries": queries, "latents": latents, "rope_key": rope_key, "w_key": w_key, "w_value": w_value, "w_out": w_out, "resid": resid, "gain_mix": gain_mix, "w_gate": w_gate, "w_up": w_up, "w_down": w_down, "gain_out": gain_out}


ROTARY_BASE = 10000.0
NORM_EPSILON = 1e-06
DEEP_ALPHA = 8.0 ** 0.25
HALF_STEP = 0.5

def rotary_tables(positions, rotary_width, grid_width):
    grid_rows = (positions // grid_width).astype(jnp.float32)
    grid_cols = (positions % grid_width).astype(jnp.float32)
    freq_count = rotary_width // 4
    inverse = ROTARY_BASE ** (-jnp.arange(freq_count, dtype=jnp.float32) / freq_count)
    angle_table = jnp.concatenate([grid_rows[:, None] * inverse, grid_cols[:, None] * inverse], axis=-1)
    return (jnp.cos(angle_table), jnp.sin(angle_table))

def rotate(vectors, cosine, sine):
    half_width = vectors.shape[-1] // 2
    leading = vectors[..., :half_width].astype(jnp.float32)
    trailing = vectors[..., half_width:].astype(jnp.float32)
    return jnp.concatenate([leading * cosine - trailing * sine, leading * sine + trailing * cosine], axis=-1).astype(jnp.bfloat16)

def widened(tensor):
    return lax.optimization_barrier(tensor.astype(jnp.bfloat16)).astype(jnp.float32)

def layer_norm(rows_in, gain_row):
    row_mean = lax.optimization_barrier(jnp.mean(rows_in, axis=1, keepdims=True))
    variance = lax.optimization_barrier(jnp.mean(rows_in * rows_in, axis=1, keepdims=True)) - row_mean * row_mean
    return ((rows_in - row_mean) * lax.rsqrt(variance + NORM_EPSILON) * gain_row.astype(jnp.float32)).astype(jnp.bfloat16)

def group_sum(left, right, group_width):
    total_sum = jnp.zeros((left.shape[0], right.shape[1]), jnp.float32)
    for group_index in range(N_TP):
        lower = group_index * group_width
        partial_term = jnp.dot(left[:, lower:lower + group_width], right[lower:lower + group_width], preferred_element_type=jnp.float32)
        total_sum = total_sum + widened(partial_term)
    return total_sum

def reference(queries, latents, rope_key, w_key, w_value, w_out, resid, gain_mix, w_gate, w_up, w_down, gain_out):
    positions = jnp.arange(TOKENS, dtype=jnp.int32)
    cosine, sine = rotary_tables(positions, ROPE, GRID_W)
    key_rot = lax.optimization_barrier(rotate(rope_key, cosine, sine)).astype(jnp.float32)
    shaped = queries.reshape(TOKENS, HEADS, NOPE + ROPE)
    q_nope = shaped[:, :, :NOPE]
    q_rot = rotate(shaped[:, :, NOPE:], cosine[:, None, :], sine[:, None, :])
    key_nope = widened(jnp.dot(latents, w_key, preferred_element_type=jnp.float32)).reshape(TOKENS, HEADS, NOPE)
    head_values = widened(jnp.dot(latents, w_value, preferred_element_type=jnp.float32)).reshape(TOKENS, HEADS, VDIM)
    block_rows = math.gcd(TOKENS, 512)
    score_scale = (NOPE + ROPE) ** (-0.5)

    def attend(block_index):
        first_row = (block_index * block_rows).astype(jnp.int32)
        query_nope = lax.dynamic_slice_in_dim(q_nope, first_row, block_rows, 0).astype(jnp.float32)
        query_rope = lax.dynamic_slice_in_dim(q_rot, first_row, block_rows, 0).astype(jnp.float32)
        scores = jnp.einsum('qhd,khd->hqk', query_nope, key_nope) + jnp.einsum('qhd,kd->hqk', query_rope, key_rot)
        scores = scores * score_scale
        row_max = lax.optimization_barrier(jnp.max(scores, axis=-1, keepdims=True))
        weights = jnp.exp(scores - row_max)
        totals = lax.optimization_barrier(jnp.sum(weights, axis=-1))
        prob_weights = widened(weights)
        heads_block = jnp.einsum('hqk,khd->qhd', prob_weights, head_values) / jnp.transpose(totals)[:, :, None]
        return heads_block.astype(jnp.bfloat16).reshape(block_rows, HEADS * VDIM)
    heads_out = lax.map(attend, jnp.arange(TOKENS // block_rows, dtype=jnp.int32)).reshape(TOKENS, HEADS * VDIM)
    attn_sum = group_sum(heads_out, w_out, HEADS * VDIM // N_TP)
    mixed_in = DEEP_ALPHA * resid.astype(jnp.float32) + attn_sum
    hidden_in = layer_norm(mixed_in, gain_mix)
    gate_sum = jnp.dot(hidden_in, w_gate, preferred_element_type=jnp.float32)
    up_sum = jnp.dot(hidden_in, w_up, preferred_element_type=jnp.float32)
    hidden = (jax.nn.silu(gate_sum) * up_sum).astype(jnp.bfloat16)
    mixer_sum = group_sum(hidden, w_down, FF // N_TP)
    return layer_norm(DEEP_ALPHA * hidden_in.astype(jnp.float32) + HALF_STEP * mixer_sum, gain_out)
```

```python
import jax
import jax.numpy as jnp
from jax import lax
from jax.experimental import pallas as pl
from jax.experimental.pallas import tpu as pltpu
from jax.sharding import PartitionSpec as P

MESH = pl.DeviceIdType.MESH
F32 = jnp.float32
BF = jnp.bfloat16

HD = 64
ROPE = 32
GRID_W = 64
ROTARY_BASE = 10000.0
EPS = 1e-06
ALPHA = 8.0**0.25
HALF = 0.5
NZ, NX, NY = 8, 4, 4
T = 192
TQ = 48
NQ = 768
QB = 256
D = 2048
FC = 768
SCALE = (1.4426950408889634) * (96.0**-0.5)


class Ring:
    def __init__(self, n, pos, dev, blk, half, sems, log):
        self.n, self.pos, self.dev = n, pos, dev
        self.blk, self.half, self.sems, self.log = blk, half, sems, log

    def at(self, k):
        return lax.rem(self.pos + (k + 2 * self.n), self.n)

    def copy(self, ref, d, t):
        ss, rs = self.sems[d]
        return pltpu.make_async_remote_copy(
            src_ref=ref,
            dst_ref=ref,
            send_sem=ss.at[t],
            recv_sem=rs.at[t],
            device_id=self.dev(self.at(1 if d == 0 else -1)),
            device_id_type=MESH,
        )

    def send(self, ref, d, t):
        cp = self.copy(ref, d, t)
        cp.start()
        self.log.append(cp)

    def start(self):
        for d in (0, 1):
            self.send(self.blk(self.pos), d, 0)

    def arrived(self, d, t):
        return self.at(-t if d == 0 else t)

    def step(self, t):
        last = self.n // 2
        for d in (0, 1):
            p = self.arrived(d, t)
            if t < last:
                self.copy(self.blk(p), d, t - 1).wait_recv()
                self.send(self.blk(p) if t < last - 1 else self.half(p, d), d, t)
            else:
                self.copy(self.half(p, d), d, t - 1).wait_recv()


def kernel(
    q_ref, lat_ref, rk_ref, wk_ref, wv_ref, wo_ref, res_ref, gm_ref, wg_ref, wu_ref, wd_ref, go_ref, cs_ref, sn_ref,
    out_ref,
    kvsend, qsend, kvr, qin, rhs, kvt, sbuf, pbuf, obuf, mbuf, osend, hb, wo, resb, gsend, gains,
    wgu, wdt, hid, mixed, part, prec, outs, orec,
    s_kvx, r_kvx, s_qx, r_qx, s_res, r_res, s_g, r_g,
    s_zkv, r_zkv, s_dkv, r_dkv, s_zgu, r_zgu, s_xgu, r_xgu, s_dgu, r_dgu,
    s_xwd, r_xwd, s_zwd, r_zwd, s_dwd, r_dwd, s_ywo, r_ywo, s_dwo, r_dwo,
    s_o, r_o, s_yh, r_yh, s_p, r_p, s_f, r_f,
):
    sp = lax.axis_index("sp")
    y = lax.axis_index("tp")
    c = lax.rem(sp, 2)
    x = lax.rem(sp // 2, NX)
    z = sp // (2 * NX)
    log = []

    def dev(zz, xx, cc, yy):
        return ((zz * NX + xx) * 2 + cc, yy)

    def mod4(v):
        return lax.rem(v + 8, 4)

    partner = dev(z, x, 1 - c, y)

    def rcopy(src, dst, ss, rs, to):
        return pltpu.make_async_remote_copy(
            src_ref=src, dst_ref=dst, send_sem=ss, recv_sem=rs, device_id=to, device_id_type=MESH
        )

    def go(cp):
        cp.start()
        log.append(cp)

    def come(ref, ss, rs):
        rcopy(ref, ref, ss, rs, partner).wait_recv()

    barrier = pltpu.get_barrier_semaphore()
    peers = [dev(z, mod4(x + dx), c, mod4(y + dy)) for dx in range(4) for dy in range(4) if dx or dy]
    peers += [dev(lax.rem(z + 1, NZ), x, c, y), dev(lax.rem(z + NZ - 1, NZ), x, c, y), partner]
    for peer in peers:
        pl.semaphore_signal(barrier, inc=1, device_id=peer, device_id_type=MESH)

    cs, sn = cs_ref[...], sn_ref[...]

    def rotated(t):
        swapped = jnp.concatenate([t[:, ROPE // 2 :], t[:, : ROPE // 2]], axis=1)
        return t * cs + swapped * sn

    lat = lat_ref[...]
    k = jnp.dot(lat, wk_ref[...], preferred_element_type=F32)
    v = jnp.dot(lat, wv_ref[...], preferred_element_type=F32)
    kr = rotated(rk_ref[...].astype(F32))
    krp = jnp.concatenate([kr[TQ * i : TQ * i + TQ] for i in range(4)], axis=1).astype(BF)
    for h in range(4):
        kv = jnp.concatenate([k[:, HD * h : HD * h + HD], v[:, HD * h : HD * h + HD]], axis=1).astype(BF)
        for i in range(4):
            kvsend[h, i] = kv[TQ * i : TQ * i + TQ]
        kvsend[h, 4] = krp
    q = q_ref[...].astype(F32)
    for h in range(4):
        qh = q[:, 96 * h : 96 * h + 96]
        full = jnp.concatenate([qh[:, :HD], rotated(qh[:, HD:]), jnp.zeros((T, 32), F32)], axis=1)
        qsend[h] = full.astype(BF)
    gsend[0] = gm_ref[...]
    gsend[1] = go_ref[...]
    wgu[0, z, x, c] = wg_ref[...]
    wgu[1, z, x, c] = wu_ref[...]
    wdt[z, x, c] = jnp.transpose(wd_ref[...].astype(F32)).astype(BF)
    wo[y] = wo_ref[...]

    pl.semaphore_wait(barrier, len(peers))

    for dx in range(1, 4):
        xt = mod4(x + dx)
        to = dev(z, xt, c, y)
        go(rcopy(kvsend.at[xt], kvr.at[z, c, :, pl.ds(TQ * x, TQ), :], s_kvx.at[dx - 1], r_kvx.at[dx - 1], to))
    for dx in range(1, 4):
        xt = mod4(x + dx)
        to = dev(z, xt, c, y)
        go(rcopy(qsend.at[xt], qin.at[x], s_qx.at[dx - 1], r_qx.at[dx - 1], to))
    kvr[z, c, :, pl.ds(pl.multiple_of(TQ * x, 16), TQ), :] = kvsend[x]
    qin[x] = qsend[x]

    zdev = lambda p: dev(p, x, c, y)
    xdev = lambda p: dev(z, p, c, y)
    ydev = lambda p: dev(z, x, c, p)
    ring_kv = Ring(
        NZ, z, zdev,
        lambda p: kvr.at[p, c],
        lambda p, h: kvr.at[p, c, :, pl.ds(96 * h, 96), :],
        [(s_zkv.at[0], r_zkv.at[0]), (s_zkv.at[1], r_zkv.at[1])], log,
    )
    ring_gu = Ring(
        NZ, z, zdev,
        lambda p: wgu.at[:, p, x, c],
        lambda p, h: wgu.at[:, p, x, c, pl.ds(16 * h, 16), :],
        [(s_zgu.at[0], r_zgu.at[0]), (s_zgu.at[1], r_zgu.at[1])], log,
    )
    ring_wd = Ring(
        NX, x, xdev,
        lambda p: wdt.at[z, p, c],
        lambda p, h: wdt.at[z, p, c, pl.ds(16 * h, 16), :],
        [(s_xwd.at[0], r_xwd.at[0]), (s_xwd.at[1], r_xwd.at[1])], log,
    )
    ring_wdz = Ring(
        NZ, z, zdev,
        lambda p: wdt.at[p, :, c],
        lambda p, h: wdt.at[p, pl.ds(2 * h, 2), c],
        [(s_zwd.at[0], r_zwd.at[0]), (s_zwd.at[1], r_zwd.at[1])], log,
    )
    ring_wo = Ring(
        NY, y, ydev,
        lambda p: wo.at[p, pl.ds(pl.multiple_of(128 * c, 128), 128), :],
        lambda p, h: wo.at[p, pl.ds(pl.multiple_of(128 * c + 64 * h, 64), 64), :],
        [(s_ywo.at[0], r_ywo.at[0]), (s_ywo.at[1], r_ywo.at[1])], log,
    )

    def gu_ring(k):
        p = lax.rem(z + k + NZ, NZ)
        return Ring(
            NX, x, xdev,
            lambda q: wgu.at[:, p, q, c],
            lambda q, h: wgu.at[:, p, q, c, pl.ds(16 * h, 16), :],
            [(s_xgu.at[k % NZ, 0], r_xgu.at[k % NZ, 0]), (s_xgu.at[k % NZ, 1], r_xgu.at[k % NZ, 1])], log,
        )

    xrings = {k: gu_ring(k) for k in (0, -1, 1, -2, 2, -3, 3, 4)}

    def to_partner(ref, ss, rs):
        go(rcopy(ref, ref, ss, rs, partner))

    from_partner = come

    def zk(k):
        return lax.rem(z + k + NZ, NZ)

    ring_gu.start()
    ring_wd.start()
    xrings[0].start()

    for dy in range(1, 4):
        yt = mod4(y + dy)
        to = dev(z, x, c, yt)
        go(rcopy(res_ref.at[pl.ds(pl.multiple_of(TQ * yt, 16), TQ), :], resb.at[y], s_res.at[dy - 1], r_res.at[dy - 1], to))
        go(rcopy(gsend, gains.at[y], s_g.at[dy - 1], r_g.at[dy - 1], to))
    resb[y] = res_ref[pl.ds(pl.multiple_of(TQ * y, 16), TQ), :]
    gains[y] = gsend[...]
    ring_wo.start()

    for dx in range(1, 4):
        xf = mod4(x - dx)
        come(kvr.at[z, c, :, pl.ds(TQ * xf, TQ), :], s_kvx.at[dx - 1], r_kvx.at[dx - 1])
    ring_kv.start()

    def kv_out(k):
        to_partner(kvr.at[zk(k), c], s_dkv.at[k % NZ], r_dkv.at[k % NZ])

    def kv_in(k):
        from_partner(kvr.at[zk(k), 1 - c], s_dkv.at[k % NZ], r_dkv.at[k % NZ])

    kv_out(0)

    kvt[...] = jnp.ones_like(kvt)
    obuf[...] = jnp.zeros_like(obuf)
    mbuf[...] = jnp.full_like(mbuf, -1e30)
    for dx in range(1, 4):
        xf = mod4(x - dx)
        come(qin.at[xf], s_qx.at[dx - 1], r_qx.at[dx - 1])
    rhs[...] = jnp.zeros_like(rhs)
    qt = jnp.transpose(qin[...].reshape(NQ, 128).astype(F32)).astype(BF)
    for i in range(4):
        rhs[i, 0:HD] = qt[0:HD]
        rhs[i, 128 + 32 * i : 160 + 32 * i] = qt[HD : HD + 32]

    def attend(p):
        for cc in range(2):
            t = jnp.transpose(kvr[p, cc, 0:4].reshape(NQ, 128).astype(F32))
            kvt[cc, HD:128] = t[HD:128].astype(BF)

        def one(qb, carry):
            qs = pl.ds(pl.multiple_of(qb * QB, QB), QB)
            mx = None
            for cc in range(2):
                krb = kvr[p, cc, 4]
                for i in range(4):
                    lhs = jnp.concatenate([kvr[p, cc, i], krb], axis=1)
                    s = jnp.dot(lhs, rhs[i, :, qs], preferred_element_type=F32)
                    r = (cc * 4 + i) * T
                    sbuf[r : r + T] = s
                    part_max = jnp.max(s.reshape(T // 8, 8, QB), axis=0)
                    mx = part_max if mx is None else jnp.maximum(mx, part_max)
            m_old = mbuf[0:1, qs]
            m_new = jnp.maximum(m_old, jnp.max(mx, axis=0, keepdims=True))
            mbuf[0:1, qs] = m_new
            factor = jnp.exp2((m_old - m_new) * SCALE)
            shift = m_new * SCALE
            acc = None
            for cc in range(2):
                for i in range(4):
                    r = (cc * 4 + i) * T
                    pbuf[r : r + T] = jnp.exp2(sbuf[r : r + T] * SCALE - shift).astype(BF)
                got = jnp.dot(kvt[cc], pbuf[cc * NQ : cc * NQ + NQ], preferred_element_type=F32)
                acc = got if acc is None else acc + got
            obuf[:, qs] = obuf[:, qs] * factor + acc
            return carry

        lax.fori_loop(0, NQ // QB, one, 0)

    def gu_out(k):
        to_partner(wgu.at[:, zk(k), :, c], s_dgu.at[k % NZ], r_dgu.at[k % NZ])

    def gu_in(k):
        from_partner(wgu.at[:, zk(k), :, 1 - c], s_dgu.at[k % NZ], r_dgu.at[k % NZ])

    def wd_out(k):
        to_partner(wdt.at[zk(k), :, c], s_dwd.at[k % NZ], r_dwd.at[k % NZ])

    def wd_in(k):
        from_partner(wdt.at[zk(k), :, 1 - c], s_dwd.at[k % NZ], r_dwd.at[k % NZ])

    def wo_out(k):
        to_partner(ring_wo.blk(ring_wo.at(k)), s_dwo.at[k % NY - 1], r_dwo.at[k % NY - 1])

    def wo_in(k):
        p = ring_wo.at(k)
        ref = wo.at[p, pl.ds(pl.multiple_of(128 - 128 * c, 128), 128), :]
        from_partner(ref, s_dwo.at[k % NY - 1], r_dwo.at[k % NY - 1])

    ring_wd.step(1)
    kv_in(0)
    attend(z)
    for t in range(1, 5):
        ks = (-t, t) if t < 4 else (4,)
        ring_kv.step(t)
        for kk in ks:
            kv_out(kk)
        ring_gu.step(t)
        for kk in ks:
            xrings[kk].start()
        if t == 1:
            ring_wd.step(2)
            xrings[0].step(1)
        if t == 2:
            xrings[0].step(2)
            gu_out(0)
            xrings[-1].step(1)
            xrings[1].step(1)
            ring_wo.step(1)
            wo_out(-1)
            wo_out(1)
        if t == 3:
            xrings[-1].step(2)
            gu_out(-1)
            xrings[1].step(2)
            gu_out(1)
            xrings[-2].step(1)
            xrings[2].step(1)
        if t == 4:
            xrings[-2].step(2)
            gu_out(-2)
            xrings[2].step(2)
            gu_out(2)
            xrings[-3].step(1)
            xrings[3].step(1)
            ring_wo.step(2)
            wo_out(2)
            ring_wdz.start()
            wd_out(0)
        for kk in ks:
            kv_in(kk)
            attend(zk(kk))

    par = lax.rem(x, 2)
    on = obuf[HD:128] / obuf[0:1]
    par_f = par.astype(F32)
    full = jnp.concatenate([on * (1.0 - par_f), on * par_f], axis=0)
    osend[...] = jnp.transpose(full).astype(BF).reshape(4, T, 128)
    for dx in range(4):
        for dy in range(4):
            if dx or dy:
                xt, yt = mod4(x + dx), mod4(y + dy)
                n = dx * 4 + dy - 1
                src = osend.at[xt, pl.ds(pl.multiple_of(TQ * yt, 16), TQ), :]
                go(rcopy(src, hb.at[4 * y + x], s_o.at[n], r_o.at[n], dev(z, xt, c, yt)))
    hb[4 * y + x] = osend[x, pl.ds(pl.multiple_of(TQ * y, 16), TQ), :]
    xrings[-3].step(2)
    gu_out(-3)
    xrings[3].step(2)
    gu_out(3)
    xrings[4].step(1)
    ring_wdz.step(1)
    wd_out(-1)
    wd_out(1)
    for kk in (-1, 1, 2):
        wo_in(kk)
    for dy in range(1, 4):
        yf = mod4(y - dy)
        come(resb.at[yf], s_res.at[dy - 1], r_res.at[dy - 1])
        come(gains.at[yf], s_g.at[dy - 1], r_g.at[dy - 1])
    for dx in range(4):
        for dy in range(4):
            if dx or dy:
                n = dx * 4 + dy - 1
                slot = 4 * mod4(y - dy) + mod4(x - dx)
                come(hb.at[slot], s_o.at[n], r_o.at[n])

    def gain(n):
        return jnp.concatenate([gains[g, n] for g in range(4)], axis=1)

    def normed(rows, gain_row):
        mean = jnp.sum(rows, axis=1, keepdims=True) * (1.0 / D)
        var = jnp.sum(rows * rows, axis=1, keepdims=True) * (1.0 / D) - mean * mean
        return ((rows - mean) * lax.rsqrt(var + EPS) * gain_row).astype(BF)

    attn = None
    for g in range(4):
        pairs = [hb[4 * g + 2 * j] + hb[4 * g + 2 * j + 1] for j in range(2)]
        term = jnp.dot(jnp.concatenate(pairs, axis=1), wo[g], preferred_element_type=F32)
        term = term.astype(BF).astype(F32)
        attn = term if attn is None else attn + term
    res = jnp.concatenate([resb[g] for g in range(4)], axis=1).astype(F32)
    hid[y] = normed(ALPHA * res + attn, gain(0))

    ring_h = Ring(
        NY, y, ydev,
        lambda p: hid.at[p],
        lambda p, h: hid.at[p, :, pl.ds(1024 * h, 1024)],
        [(s_yh.at[0], r_yh.at[0]), (s_yh.at[1], r_yh.at[1])], log,
    )
    ring_h.start()
    xrings[4].step(2)
    gu_out(4)
    ring_wdz.step(2)
    wd_out(-2)
    wd_out(2)
    ring_h.step(1)
    for kk in (0, -1, 1, -2, 2, -3, 3, 4):
        gu_in(kk)
    ring_wdz.step(3)
    wd_out(-3)
    wd_out(3)
    ring_h.step(2)

    rows = hid[...].reshape(T, D)

    def gate_up(j, carry):
        cols = pl.ds(pl.multiple_of(j * QB, QB), QB)
        gate = jnp.dot(rows, wgu[0, :, :, :, :, cols].reshape(D, QB), preferred_element_type=F32)
        up = jnp.dot(rows, wgu[1, :, :, :, :, cols].reshape(D, QB), preferred_element_type=F32)
        mixed[:, cols] = (gate / (1.0 + jnp.exp(-gate)) * up).astype(BF)
        return carry

    lax.fori_loop(0, FC // QB, gate_up, 0)
    ring_wdz.step(4)
    wd_out(4)
    for kk in (0, -1, 1, -2, 2, -3, 3, 4):
        wd_in(kk)
    units = mixed[...]

    def down(j, carry):
        w = wdt[j].reshape(QB, FC)
        got = lax.dot_general(units, w, (((1,), (1,)), ((), ())), preferred_element_type=F32)
        part[:, :, pl.ds(pl.multiple_of(j * QB, QB), QB)] = got.astype(BF).reshape(4, TQ, QB)
        return carry

    lax.fori_loop(0, NZ, down, 0)
    for dy in range(1, 4):
        yt = mod4(y + dy)
        go(rcopy(part.at[yt], prec.at[dy - 1], s_p.at[dy - 1], r_p.at[dy - 1], dev(z, x, c, yt)))
    total = part[y].astype(F32)
    for dy in range(1, 4):
        come(prec.at[dy - 1], s_p.at[dy - 1], r_p.at[dy - 1])
        total = total + prec[dy - 1].astype(F32)
    outs[...] = normed(ALPHA * hid[y].astype(F32) + HALF * total, gain(1))
    for dy in range(1, 4):
        yt = mod4(y + dy)
        src = outs.at[:, pl.ds(pl.multiple_of(512 * yt, 512), 512)]
        go(rcopy(src, orec.at[y], s_f.at[dy - 1], r_f.at[dy - 1], dev(z, x, c, yt)))
    orec[y] = outs[:, pl.ds(pl.multiple_of(512 * y, 512), 512)]
    for dy in range(1, 4):
        yf = mod4(y - dy)
        come(orec.at[yf], s_f.at[dy - 1], r_f.at[dy - 1])
    out_ref[...] = orec[...].reshape(T, 512)
    for cp in log:
        cp.wait_send()


def local(queries, latents, rope_key, w_key, w_value, w_out, resid, gain_mix, w_gate, w_up, w_down, gain_out):
    start = lax.axis_index("sp") * T
    positions = start + jnp.arange(T, dtype=jnp.int32)
    grid_rows = (positions // GRID_W).astype(F32)
    grid_cols = (positions % GRID_W).astype(F32)
    count = ROPE // 4
    inverse = ROTARY_BASE ** (-jnp.arange(count, dtype=F32) / count)
    angles = jnp.concatenate([grid_rows[:, None] * inverse, grid_cols[:, None] * inverse], axis=-1)
    cos, sin = jnp.cos(angles), jnp.sin(angles)
    cs = jnp.concatenate([cos, cos], axis=1)
    sn = jnp.concatenate([-sin, sin], axis=1)
    dma = pltpu.SemaphoreType.DMA
    V = pltpu.VMEM

    def pair(*shape):
        return [dma(shape), dma(shape)]

    sems = []
    for shape in (
        (3,), (3,), (3,), (3,),
        (2, 4), (8,), (2, 4), (8, 2, 2), (8,),
        (2, 2), (2, 4), (8,), (2, 2), (3,),
        (15,), (2, 2), (3,), (3,),
    ):
        sems += pair(*shape)
    scratch = [
        V((4, 5, TQ, 128), BF),
        V((4, T, 128), BF),
        V((NZ, 2, 5, T, 128), BF),
        V((4, T, 128), BF),
        V((4, 256, NQ), BF),
        V((2, 128, NQ), BF),
        V((8 * T, QB), F32),
        V((8 * T, QB), BF),
        V((128, NQ), F32),
        V((8, NQ), F32),
        V((4, T, 128), BF),
        V((16, TQ, 128), BF),
        V((NY, 256, D), BF),
        V((NY, TQ, 512), BF),
        V((2, 1, 512), F32),
        V((NY, 2, 1, 512), F32),
        V((2, NZ, NX, 2, 32, FC), BF),
        V((NZ, NX, 2, 32, FC), BF),
        V((NY, TQ, D), BF),
        V((T, FC), BF),
        V((NY, TQ, D), BF),
        V((3, TQ, D), BF),
        V((TQ, D), BF),
        V((NY, TQ, 512), BF),
    ]
    vm = pl.BlockSpec(memory_space=pltpu.VMEM)
    return pl.pallas_call(
        kernel,
        out_shape=jax.ShapeDtypeStruct((T, 512), BF),
        in_specs=[vm] * 14,
        out_specs=vm,
        scratch_shapes=scratch + sems,
        compiler_params=pltpu.CompilerParams(
            collective_id=0, has_side_effects=True, vmem_limit_bytes=60 * 1024 * 1024
        ),
    )(
        queries, latents, rope_key, w_key, w_value, w_out, resid, gain_mix.reshape(1, 512),
        w_gate, w_up, w_down, gain_out.reshape(1, 512), cs, sn,
    )


def solution(mesh):
    placed = (
        P("sp", "tp"), P("sp", None), P("sp", None), P(None, "tp"), P(None, "tp"), P("tp", None),
        P("sp", "tp"), P("tp"), P("sp", "tp"), P("sp", "tp"), P("tp", "sp"), P("tp"),
    )
    return jax.shard_map(local, mesh=mesh, in_specs=placed, out_specs=P("sp", "tp"), check_vma=False)
```

```python
import jax
import jax.numpy as jnp
from jax import lax
from jax.experimental import pallas as pl
from jax.experimental.pallas import tpu as pltpu
from jax.sharding import PartitionSpec as P

MESH = pl.DeviceIdType.MESH
F32 = jnp.float32
BF = jnp.bfloat16

HD = 64
ROPE = 32
GRID_W = 64
ROTARY_BASE = 10000.0
EPS = 1e-06
ALPHA = 8.0**0.25
HALF = 0.5
NZ, NX, NY = 8, 4, 4
T = 192
TQ = 48
NQ = 768
QB = 256
D = 2048
FC = 768
SCALE = (1.4426950408889634) * (96.0**-0.5)


class Ring:
    def __init__(self, n, pos, dev, blk, half, sems, log, pieces=False):
        self.n, self.pos, self.dev, self.pieces = n, pos, dev, pieces
        self.blk, self.half, self.sems, self.log = blk, half, sems, log

    def at(self, k):
        return lax.rem(self.pos + (k + 2 * self.n), self.n)

    def copy(self, p, d, t, h):
        ss, rs = self.sems[d]
        ref = self.blk(p) if h is None else self.half(p, h)
        at = (t, h) if self.pieces else (t,)
        return pltpu.make_async_remote_copy(
            src_ref=ref,
            dst_ref=ref,
            send_sem=ss.at[at],
            recv_sem=rs.at[at],
            device_id=self.dev(self.at(1 if d == 0 else -1)),
            device_id_type=MESH,
        )

    def parts(self, t):
        if t == self.n // 2 - 1:
            return ((0, 0), (1, 1))
        if self.pieces:
            return ((0, 0), (1, 1), (0, 1), (1, 0))
        return ((0, None), (1, None))

    def send(self, p, d, t, h):
        cp = self.copy(p, d, t, h)
        cp.start()
        self.log.append(cp)

    def start(self):
        for d, h in self.parts(0):
            self.send(self.pos, d, 0, h)

    def arrived(self, d, t):
        return self.at(-t if d == 0 else t)

    def take(self, t):
        for d, h in self.parts(t - 1):
            self.copy(self.arrived(d, t), d, t - 1, h).wait_recv()

    def pass_on(self, t):
        for d, h in self.parts(t):
            self.send(self.arrived(d, t), d, t, h)

    def step(self, t):
        for d, h in self.parts(t - 1):
            p = self.arrived(d, t)
            self.copy(p, d, t - 1, h).wait_recv()
            if self.pieces and t < self.n // 2 and (d, h) in self.parts(t):
                self.send(p, d, t, h)
        if not self.pieces and t < self.n // 2:
            self.pass_on(t)


def kernel(
    q_ref, lat_ref, rk_ref, wk_ref, wv_ref, wo_ref, res_ref, gm_ref, wg_ref, wu_ref, wd_ref, go_ref, cs_ref, sn_ref,
    out_ref,
    kvsend, qsend, kvr, qin, qt, kp, kvt, sbuf, pbuf, obuf, mbuf, osend, hb, wo, resb, gains,
    wgu, wdt, hid, mixed, part, crec, stat,
    s_kvx, r_kvx, s_qx, r_qx, s_res, r_res, s_g, r_g,
    s_zkv, r_zkv, s_dkv, r_dkv, s_zgu, r_zgu, s_xgu, r_xgu, s_dgu, r_dgu,
    s_xwd, r_xwd, s_zwd, r_zwd, s_dwd, r_dwd, s_ywo, r_ywo, s_dwo, r_dwo,
    s_o, r_o, s_yh, r_yh, s_p, r_p, s_f, r_f,
):
    sp = lax.axis_index("sp")
    y = lax.axis_index("tp")
    c = lax.rem(sp, 2)
    x = lax.rem(sp // 2, NX)
    z = sp // (2 * NX)
    log = []

    def dev(zz, xx, cc, yy):
        return ((zz * NX + xx) * 2 + cc, yy)

    def mod4(v):
        return lax.rem(v + 8, 4)

    def zk(k):
        return lax.rem(z + k + NZ, NZ)

    partner = dev(z, x, 1 - c, y)

    def rcopy(src, dst, ss, rs, to):
        return pltpu.make_async_remote_copy(
            src_ref=src, dst_ref=dst, send_sem=ss, recv_sem=rs, device_id=to, device_id_type=MESH
        )

    def go(cp):
        cp.start()
        log.append(cp)

    def come(ref, ss, rs):
        rcopy(ref, ref, ss, rs, partner).wait_recv()

    def to_partner(ref, ss, rs):
        go(rcopy(ref, ref, ss, rs, partner))

    def rows48(i):
        return pl.ds(pl.multiple_of(TQ * i, 16), TQ)

    def cols512(i):
        return pl.ds(pl.multiple_of(512 * i, 512), 512)

    barrier = pltpu.get_barrier_semaphore()
    peers = [dev(z, mod4(x + dx), c, mod4(y + dy)) for dx in range(4) for dy in range(4) if dx or dy]
    peers += [dev(zk(1), x, c, y), dev(zk(-1), x, c, y), partner]
    for peer in peers:
        pl.semaphore_signal(barrier, inc=1, device_id=peer, device_id_type=MESH)

    wgu[0, z, x, c] = wg_ref[...]
    wgu[1, z, x, c] = wu_ref[...]
    wdt[z, x, c] = wd_ref[...]
    wo[y] = wo_ref[...]
    gains[y, 0] = gm_ref[...]
    gains[y, 1] = go_ref[...]
    lat = lat_ref[...]
    k = jnp.dot(lat, wk_ref[...], preferred_element_type=F32)
    v = jnp.dot(lat, wv_ref[...], preferred_element_type=F32)
    cst, snt, rkt = cs_ref[...], sn_ref[...], rk_ref[...].astype(F32)
    swapped = jnp.concatenate([rkt[ROPE // 2 :], rkt[: ROPE // 2]], axis=0)
    krt = rkt * cst + swapped * snt
    table = jnp.transpose(jnp.concatenate([cst, snt, krt, krt], axis=0))
    kr = table[:, 2 * ROPE : 3 * ROPE]
    krp = jnp.concatenate([kr[TQ * i : TQ * i + TQ] for i in range(4)], axis=1).astype(BF)
    for h in range(4):
        kv = jnp.concatenate([k[:, HD * h : HD * h + HD], v[:, HD * h : HD * h + HD]], axis=1).astype(BF)
        for i in range(4):
            kvsend[h, i] = kv[TQ * i : TQ * i + TQ]
        kvsend[h, 4] = krp

    zdev = lambda p: dev(p, x, c, y)
    xdev = lambda p: dev(z, p, c, y)
    ydev = lambda p: dev(z, x, c, p)

    def pairs(ss, rs):
        return [(ss.at[d], rs.at[d]) for d in (0, 1)]

    ring_kv = Ring(
        NZ, z, zdev,
        lambda p: kvr.at[p, c],
        lambda p, h: kvr.at[p, c, :, pl.ds(96 * h, 96), :],
        pairs(s_zkv, r_zkv), log, pieces=True,
    )
    ring_gu = Ring(
        NZ, z, zdev,
        lambda p: wgu.at[:, p, x, c],
        lambda p, h: wgu.at[:, p, x, c, pl.ds(16 * h, 16), :],
        pairs(s_zgu, r_zgu), log,
    )
    ring_wd = Ring(
        NX, x, xdev,
        lambda p: wdt.at[z, p, c],
        lambda p, h: wdt.at[z, p, c, pl.ds(16 * h, 16), :],
        pairs(s_xwd, r_xwd), log,
    )
    ring_wdz = Ring(
        NZ, z, zdev,
        lambda p: wdt.at[p, :, c],
        lambda p, h: wdt.at[p, pl.ds(2 * h, 2), c],
        pairs(s_zwd, r_zwd), log,
    )
    ring_wo = Ring(
        NY, y, ydev,
        lambda p: wo.at[p, pl.ds(pl.multiple_of(128 * c, 128), 128), :],
        lambda p, h: wo.at[p, pl.ds(pl.multiple_of(128 * c + 64 * h, 64), 64), :],
        pairs(s_ywo, r_ywo), log,
    )
    ring_h = Ring(
        NY, y, ydev,
        lambda p: hid.at[p],
        lambda p, h: hid.at[p, :, pl.ds(1024 * h, 1024)],
        pairs(s_yh, r_yh), log, pieces=True,
    )

    def gu_ring(k):
        p = zk(k)
        return Ring(
            NX, x, xdev,
            lambda q: wgu.at[:, p, q, c],
            lambda q, h: wgu.at[:, p, q, c, pl.ds(16 * h, 16), :],
            [(s_xgu.at[k % NZ, d], r_xgu.at[k % NZ, d]) for d in (0, 1)], log,
        )

    xr = {k: gu_ring(k) for k in (0, -1, 1, -2, 2, -3, 3, 4)}

    def kv_out(k):
        to_partner(kvr.at[zk(k), c], s_dkv.at[k % NZ], r_dkv.at[k % NZ])

    def kv_in(k):
        come(kvr.at[zk(k), 1 - c], s_dkv.at[k % NZ], r_dkv.at[k % NZ])

    def gu_out(k):
        to_partner(wgu.at[:, zk(k), :, c], s_dgu.at[k % NZ], r_dgu.at[k % NZ])

    def gu_in(k):
        come(wgu.at[:, zk(k), :, 1 - c], s_dgu.at[k % NZ], r_dgu.at[k % NZ])

    def wd_out(k):
        to_partner(wdt.at[zk(k), :, c], s_dwd.at[k % NZ], r_dwd.at[k % NZ])

    def wd_in(k):
        come(wdt.at[zk(k), :, 1 - c], s_dwd.at[k % NZ], r_dwd.at[k % NZ])

    def wo_out(k):
        to_partner(ring_wo.blk(ring_wo.at(k)), s_dwo.at[k % NY - 1], r_dwo.at[k % NY - 1])

    def wo_in(k):
        ref = wo.at[ring_wo.at(k), pl.ds(pl.multiple_of(128 - 128 * c, 128), 128), :]
        come(ref, s_dwo.at[k % NY - 1], r_dwo.at[k % NY - 1])

    pl.semaphore_wait(barrier, len(peers))

    ring_gu.start()
    for dx in (1, 3, 2):
        xt = mod4(x + dx)
        go(rcopy(kvsend.at[xt], kvr.at[z, c, :, rows48(x), :], s_kvx.at[dx - 1], r_kvx.at[dx - 1], xdev(xt)))
    kvr[z, c, :, rows48(x), :] = kvsend[x]
    cs, sn = table[:, :ROPE], table[:, ROPE : 2 * ROPE]
    q = q_ref[...].astype(F32)
    for h in range(4):
        qr = q[:, 96 * h + HD : 96 * h + 96]
        turned = qr * cs + jnp.concatenate([qr[:, ROPE // 2 :], qr[:, : ROPE // 2]], axis=1) * sn
        full = jnp.concatenate([q[:, 96 * h : 96 * h + HD], turned, jnp.zeros((T, 32), F32)], axis=1)
        qsend[h] = full.astype(BF)
    for dx in (1, 3, 2):
        xt = mod4(x + dx)
        go(rcopy(qsend.at[xt], qin.at[x], s_qx.at[dx - 1], r_qx.at[dx - 1], xdev(xt)))
    qin[x] = qsend[x]
    xr[0].start()
    ring_wd.start()

    for dy in (1, 3, 2):
        yt = mod4(y + dy)
        go(rcopy(res_ref.at[rows48(yt), :], resb.at[y], s_res.at[dy - 1], r_res.at[dy - 1], ydev(yt)))
        go(rcopy(gains.at[y], gains.at[y], s_g.at[dy - 1], r_g.at[dy - 1], ydev(yt)))
    resb[y] = res_ref[rows48(y), :]
    ring_wo.start()

    ring_gu.step(1)
    for dx in (1, 3, 2):
        come(kvr.at[z, c, :, rows48(mod4(x - dx)), :], s_kvx.at[dx - 1], r_kvx.at[dx - 1])
    ring_kv.start()
    kv_out(0)
    xr[-1].start()
    xr[1].start()

    kvt[...] = jnp.ones_like(kvt)
    obuf[...] = jnp.zeros_like(obuf)
    mbuf[...] = jnp.full_like(mbuf, -1e30)
    for dx in (1, 3, 2):
        come(qin.at[mod4(x - dx)], s_qx.at[dx - 1], r_qx.at[dx - 1])
    qt[...] = jnp.transpose(qin[...].reshape(NQ, 128))

    def attend(p):
        for cc in range(2):
            kr = kvr[p, cc, 4]
            for i in range(4):
                lo = (cc * 4 + i) * T
                kp[lo : lo + T] = jnp.concatenate(
                    [kvr[p, cc, i][:, :HD], kr[:, ROPE * i : ROPE * i + ROPE], jnp.zeros((T, ROPE), BF)], axis=1
                )
            kvt[cc, HD:128] = jnp.transpose(kvr[p, cc, 0:4].reshape(NQ, 128))[HD:128]

        def scores(qb, j):
            s = jnp.dot(kp[T * j : T * j + T], qt[:, QB * qb : QB * qb + QB], preferred_element_type=F32)
            sbuf[qb % 2, T * j : T * j + T] = s
            return jnp.max(s.reshape(T // 8, 8, QB), axis=0)

        maxima = [scores(0, j) for j in range(8)]
        for qb in range(3):
            qs = slice(QB * qb, QB * qb + QB)
            b = qb % 2
            top = maxima[0]
            for other in maxima[1:]:
                top = jnp.maximum(top, other)
            m_old = mbuf[0:1, qs]
            m_new = jnp.maximum(m_old, jnp.max(top, axis=0, keepdims=True))
            mbuf[0:1, qs] = m_new
            factor = jnp.exp2((m_old - m_new) * SCALE)
            shift = m_new * SCALE
            maxima = []
            acc = None
            for j in range(8):
                if qb < 2:
                    maxima.append(scores(qb + 1, j))
                pbuf[b, T * j : T * j + T] = jnp.exp2(sbuf[b, T * j : T * j + T] * SCALE - shift).astype(BF)
                if j % 4 == 3:
                    cc = j // 4
                    got = jnp.dot(kvt[cc], pbuf[b, cc * NQ : cc * NQ + NQ], preferred_element_type=F32)
                    acc = got if acc is None else acc + got
            obuf[:, qs] = obuf[:, qs] * factor + acc

    kv_in(0)
    attend(z)
    ring_kv.step(1)
    kv_out(-1)
    kv_out(1)
    xr[0].step(1)
    ring_wd.step(1)
    kv_in(-1)
    attend(zk(-1))
    kv_in(1)
    attend(zk(1))
    ring_kv.step(2)
    kv_out(-2)
    kv_out(2)
    xr[0].step(2)
    gu_out(0)
    ring_wd.step(2)
    wd_out(0)
    xr[-1].step(1)
    xr[1].step(1)
    ring_gu.take(2)
    xr[-2].start()
    xr[2].start()
    kv_in(-2)
    attend(zk(-2))
    kv_in(2)
    attend(zk(2))
    ring_kv.step(3)
    kv_out(-3)
    kv_out(3)
    ring_gu.pass_on(2)
    ring_wdz.start()
    xr[-1].step(2)
    gu_out(-1)
    xr[1].step(2)
    gu_out(1)
    ring_wo.step(1)
    wo_out(-1)
    wo_out(1)
    kv_in(-3)
    attend(zk(-3))
    ring_kv.step(4)
    kv_out(4)
    xr[-2].step(1)
    xr[2].step(1)
    kv_in(3)
    attend(zk(3))
    kv_in(4)
    attend(zk(4))

    par = lax.rem(x, 2).astype(F32)
    on = obuf[HD:128] / obuf[0:1]
    full = jnp.concatenate([on * (1.0 - par), on * par], axis=0)
    osend[...] = jnp.transpose(full).astype(BF).reshape(4, T, 128)
    others = [(dx, dy) for dx in range(4) for dy in range(4) if dx or dy]
    for dx, dy in sorted(others, key=lambda o: -(min(o[0], 4 - o[0]) + min(o[1], 4 - o[1]))):
        xt, yt = mod4(x + dx), mod4(y + dy)
        n = dx * 4 + dy - 1
        go(rcopy(osend.at[xt, rows48(yt), :], hb.at[4 * y + x], s_o.at[n], r_o.at[n], dev(z, xt, c, yt)))
    hb[4 * y + x] = osend[x, rows48(y), :]
    ring_gu.step(3)
    xr[-3].start()
    xr[3].start()
    ring_wo.step(2)
    wo_out(2)
    xr[-2].step(2)
    gu_out(-2)
    xr[2].step(2)
    gu_out(2)
    for dy in (1, 3, 2):
        yf = mod4(y - dy)
        come(resb.at[yf], s_res.at[dy - 1], r_res.at[dy - 1])
        come(gains.at[yf], s_g.at[dy - 1], r_g.at[dy - 1])
    for kk in (-1, 1, 2):
        wo_in(kk)
    for dx, dy in others:
        n = dx * 4 + dy - 1
        come(hb.at[4 * mod4(y - dy) + mod4(x - dx)], s_o.at[n], r_o.at[n])

    attn = None
    for g in range(4):
        heads = [hb[4 * g + 2 * j] + hb[4 * g + 2 * j + 1] for j in range(2)]
        term = jnp.dot(jnp.concatenate(heads, axis=1), wo[g], preferred_element_type=F32)
        term = term.astype(BF).astype(F32)
        attn = term if attn is None else attn + term
    res = jnp.concatenate([resb[g] for g in range(4)], axis=1).astype(F32)
    rows = ALPHA * res + attn
    mean = jnp.sum(rows, axis=1, keepdims=True) * (1.0 / D)
    var = jnp.sum(rows * rows, axis=1, keepdims=True) * (1.0 / D) - mean * mean
    gain = jnp.concatenate([gains[g, 0] for g in range(4)], axis=1)
    hid[y] = ((rows - mean) * lax.rsqrt(var + EPS) * gain).astype(BF)

    ring_h.start()
    ring_gu.step(4)
    xr[4].start()
    xr[-3].step(1)
    xr[3].step(1)
    ring_wdz.step(1)
    wd_out(-1)
    wd_out(1)
    xr[-3].step(2)
    gu_out(-3)
    xr[3].step(2)
    gu_out(3)
    ring_h.step(1)
    xr[4].step(1)
    ring_wdz.step(2)
    wd_out(-2)
    wd_out(2)
    xr[4].step(2)
    gu_out(4)
    for kk in (0, -1, 1, -2, 2, -3, 3, 4):
        gu_in(kk)

    def gate_up(blocks, lo):
        rows = blocks[0] if len(blocks) == 1 else jnp.concatenate(blocks, axis=0)
        n = rows.shape[0]

        def one(j, carry):
            cols = pl.ds(pl.multiple_of(j * QB, QB), QB)
            gate = jnp.dot(rows, wgu[0, :, :, :, :, cols].reshape(D, QB), preferred_element_type=F32)
            up = jnp.dot(rows, wgu[1, :, :, :, :, cols].reshape(D, QB), preferred_element_type=F32)
            mixed[lo : lo + n, cols] = (gate / (1.0 + jnp.exp(-gate)) * up).astype(BF)
            return carry

        lax.fori_loop(0, FC // QB, one, 0)

    def down(slot, count):
        units = mixed[TQ * slot : TQ * (slot + count)]

        def one(j, carry):
            w = wdt[j].reshape(QB, FC)
            got = lax.dot_general(units, w, (((1,), (1,)), ((), ())), preferred_element_type=F32)
            got = got.astype(BF).reshape(count, TQ, QB)
            part[slot : slot + count, :, pl.ds(pl.multiple_of(j * QB, QB), QB)] = got
            return carry

        lax.fori_loop(0, NZ, one, 0)

    dist = (0, -1, 1, 2)

    def send_parts(slots):
        for s in slots:
            for dy in (2, 1, 3):
                yt = mod4(y + dy)
                dst = crec.at[dy - 1, mod4(y + dist[s])]
                go(rcopy(part.at[s, :, cols512(yt)], dst, s_p.at[dy - 1, s], r_p.at[dy - 1, s], ydev(yt)))

    gate_up([hid[y], hid[mod4(y - 1)], hid[mod4(y + 1)]], 0)
    ring_h.step(2)
    ring_wdz.step(3)
    wd_out(-3)
    wd_out(3)
    gate_up([hid[mod4(y + 2)]], 3 * TQ)
    ring_wdz.step(4)
    wd_out(4)
    for kk in (0, -1, 1, -2, 2, -3, 3, 4):
        wd_in(kk)
    down(0, 3)
    send_parts((0, 1, 2))
    down(3, 1)
    send_parts((3,))
    for s in range(4):
        crec[3, mod4(y + dist[s])] = part[s, :, cols512(y)]
    total = crec[3].astype(F32)
    for dy in (1, 3, 2):
        for s in range(4):
            come(crec.at[dy - 1, mod4(y - dy + dist[s])], s_p.at[dy - 1, s], r_p.at[dy - 1, s])
        total = total + crec[dy - 1].astype(F32)
    rows = (ALPHA * hid[:, :, cols512(y)].astype(F32) + HALF * total).reshape(T, 512)
    lane = lax.broadcasted_iota(jnp.int32, (T, 128), 1)
    s1 = jnp.sum(rows, axis=1, keepdims=True)
    s2 = jnp.sum(rows * rows, axis=1, keepdims=True)
    sums = jnp.where(lane == 0, s1, jnp.where(lane == 1, s2, 0.0))
    stat[0] = jnp.transpose(sums)[0:8]
    for dy in (2, 1, 3):
        go(rcopy(stat.at[0], stat.at[dy], s_f.at[dy - 1], r_f.at[dy - 1], ydev(mod4(y + dy))))
    both = stat[0]
    for dy in (1, 3, 2):
        come(stat.at[dy], s_f.at[dy - 1], r_f.at[dy - 1])
        both = both + stat[dy]
    both = jnp.transpose(jnp.concatenate([both, jnp.zeros((120, T), F32)], axis=0))
    mean = both[:, 0:1] * (1.0 / D)
    var = both[:, 1:2] * (1.0 / D) - mean * mean
    out_ref[...] = ((rows - mean) * lax.rsqrt(var + EPS) * gains[y, 1]).astype(BF)
    for cp in log:
        cp.wait_send()


def local(queries, latents, rope_key, w_key, w_value, w_out, resid, gain_mix, w_gate, w_up, w_down, gain_out):
    start = lax.axis_index("sp") * T
    positions = start + jnp.arange(T, dtype=jnp.int32)
    grid_rows = (positions // GRID_W).astype(F32)
    grid_cols = (positions % GRID_W).astype(F32)
    count = ROPE // 4
    inverse = ROTARY_BASE ** (-jnp.arange(count, dtype=F32) / count)
    angles = jnp.concatenate([inverse[:, None] * grid_rows, inverse[:, None] * grid_cols], axis=0)
    cos, sin = jnp.cos(angles), jnp.sin(angles)
    cs = jnp.concatenate([cos, cos], axis=0)
    sn = jnp.concatenate([-sin, sin], axis=0)
    dma = pltpu.SemaphoreType.DMA
    V = pltpu.VMEM

    def pair(*shape):
        return [dma(shape), dma(shape)]

    sems = []
    for shape in (
        (3,), (3,), (3,), (3,),
        (2, 4, 2), (8,), (2, 4), (8, 2, 2), (8,),
        (2, 2), (2, 4), (8,), (2, 2), (3,),
        (15,), (2, 2, 2), (3, 4), (3,),
    ):
        sems += pair(*shape)
    scratch = [
        V((4, 5, TQ, 128), BF),
        V((4, T, 128), BF),
        V((NZ, 2, 5, T, 128), BF),
        V((4, T, 128), BF),
        V((128, NQ), BF),
        V((8 * T, 128), BF),
        V((2, 128, NQ), BF),
        V((2, 8 * T, QB), F32),
        V((2, 8 * T, QB), BF),
        V((128, NQ), F32),
        V((8, NQ), F32),
        V((4, T, 128), BF),
        V((16, TQ, 128), BF),
        V((NY, 256, D), BF),
        V((NY, TQ, 512), BF),
        V((NY, 2, 1, 512), F32),
        V((2, NZ, NX, 2, 32, FC), BF),
        V((NZ, NX, 2, 32, FC), BF),
        V((NY, TQ, D), BF),
        V((T, FC), BF),
        V((NY, TQ, D), BF),
        V((NY, NY, TQ, 512), BF),
        V((NY, 8, T), F32),
    ]
    vm = pl.BlockSpec(memory_space=pltpu.VMEM)
    return pl.pallas_call(
        kernel,
        out_shape=jax.ShapeDtypeStruct((T, 512), BF),
        in_specs=[vm] * 14,
        out_specs=vm,
        scratch_shapes=scratch + sems,
        compiler_params=pltpu.CompilerParams(
            collective_id=0, has_side_effects=True, vmem_limit_bytes=60 * 1024 * 1024
        ),
    )(
        queries, latents, rope_key.T, w_key, w_value, w_out, resid, gain_mix.reshape(1, 512),
        w_gate, w_up, w_down.T, gain_out.reshape(1, 512), cs, sn,
    )


def solution(mesh):
    placed = (
        P("sp", "tp"), P("sp", None), P("sp", None), P(None, "tp"), P(None, "tp"), P("tp", None),
        P("sp", "tp"), P("tp"), P("sp", "tp"), P("sp", "tp"), P("tp", "sp"), P("tp"),
    )
    return jax.shard_map(local, mesh=mesh, in_specs=placed, out_specs=P("sp", "tp"), check_vma=False)
```

```python
import jax
import jax.numpy as jnp
from jax import lax
from jax.experimental import pallas as pl
from jax.experimental.pallas import tpu as pltpu
from jax.sharding import PartitionSpec as P

MESH = pl.DeviceIdType.MESH
F32 = jnp.float32
BF = jnp.bfloat16

HD = 64
ROPE = 32
GRID_W = 64
ROTARY_BASE = 10000.0
EPS = 1e-06
ALPHA = 8.0**0.25
HALF = 0.5
NZ, NX, NY = 8, 4, 4
T = 192
TQ = 48
NQ = 768
QB = 256
D = 2048
FC = 768
SCALE = (1.4426950408889634) * (96.0**-0.5)


class Ring:
    WHOLE = ((0, None), (1, None))
    HALVES = ((0, 0), (1, 1))

    def __init__(self, n, pos, dev, blk, half, sems, log, travel=WHOLE, last=HALVES):
        self.n, self.pos, self.dev, self.travel, self.last = n, pos, dev, travel, last
        self.blk, self.half, self.sems, self.log = blk, half, sems, log
        self.pieces = travel is not self.WHOLE

    def at(self, k):
        return lax.rem(self.pos + (k + 2 * self.n), self.n)

    def copy(self, p, d, t, h):
        ss, rs = self.sems[d]
        ref = self.blk(p) if h is None else self.half(p, h)
        at = (t, h) if self.pieces else (t,)
        return pltpu.make_async_remote_copy(
            src_ref=ref,
            dst_ref=ref,
            send_sem=ss.at[at],
            recv_sem=rs.at[at],
            device_id=self.dev(self.at(1 if d == 0 else -1)),
            device_id_type=MESH,
        )

    def parts(self, t):
        return self.last if t == self.n // 2 - 1 else self.travel

    def send(self, p, d, t, h):
        cp = self.copy(p, d, t, h)
        cp.start()
        self.log.append(cp)

    def start(self):
        for d, h in self.parts(0):
            self.send(self.pos, d, 0, h)

    def arrived(self, d, t):
        return self.at(-t if d == 0 else t)

    def take(self, t):
        for d, h in self.parts(t - 1):
            self.copy(self.arrived(d, t), d, t - 1, h).wait_recv()

    def pass_on(self, t):
        for d, h in self.parts(t):
            self.send(self.arrived(d, t), d, t, h)

    def step(self, t):
        for d, h in self.parts(t - 1):
            p = self.arrived(d, t)
            self.copy(p, d, t - 1, h).wait_recv()
            if self.pieces and t < self.n // 2 and (d, h) in self.parts(t):
                self.send(p, d, t, h)
        if not self.pieces and t < self.n // 2:
            self.pass_on(t)


def kernel(
    q_ref, lat_ref, rk_ref, wk_ref, wv_ref, wo_ref, res_ref, gm_ref, wg_ref, wu_ref, wd_ref, go_ref, cs_ref, sn_ref,
    out_ref,
    kvsend, qsend, kvr, qin, qt, kp, kvt, sbuf, pbuf, obuf, mbuf, osend, hb, wo, resb, gains,
    wgu, wdt, hid, mixed, part, crec, stat,
    s_kvx, r_kvx, s_qx, r_qx, s_res, r_res, s_g, r_g,
    s_zkv, r_zkv, s_dkv, r_dkv, s_zgu, r_zgu, s_xgu, r_xgu, s_dgu, r_dgu,
    s_xwd, r_xwd, s_zwd, r_zwd, s_dwd, r_dwd, s_ywo, r_ywo, s_dwo, r_dwo,
    s_o, r_o, s_yh, r_yh, s_p, r_p, s_f, r_f,
):
    sp = lax.axis_index("sp")
    y = lax.axis_index("tp")
    c = lax.rem(sp, 2)
    x = lax.rem(sp // 2, NX)
    z = sp // (2 * NX)
    log = []

    def dev(zz, xx, cc, yy):
        return ((zz * NX + xx) * 2 + cc, yy)

    def mod4(v):
        return lax.rem(v + 8, 4)

    def zk(k):
        return lax.rem(z + k + NZ, NZ)

    partner = dev(z, x, 1 - c, y)

    def rcopy(src, dst, ss, rs, to):
        return pltpu.make_async_remote_copy(
            src_ref=src, dst_ref=dst, send_sem=ss, recv_sem=rs, device_id=to, device_id_type=MESH
        )

    def go(cp):
        cp.start()
        log.append(cp)

    def come(ref, ss, rs):
        rcopy(ref, ref, ss, rs, partner).wait_recv()

    def to_partner(ref, ss, rs):
        go(rcopy(ref, ref, ss, rs, partner))

    def rows48(i):
        return pl.ds(pl.multiple_of(TQ * i, 16), TQ)

    def cols512(i):
        return pl.ds(pl.multiple_of(512 * i, 512), 512)

    barrier = pltpu.get_barrier_semaphore()
    peers = [dev(z, mod4(x + dx), c, mod4(y + dy)) for dx in range(4) for dy in range(4) if dx or dy]
    peers += [dev(zk(1), x, c, y), dev(zk(-1), x, c, y), partner]
    for peer in peers:
        pl.semaphore_signal(barrier, inc=1, device_id=peer, device_id_type=MESH)

    wgu[0, z, x, c] = wg_ref[...]
    wgu[1, z, x, c] = wu_ref[...]
    wdt[z, x, c] = wd_ref[...]
    wo[y] = wo_ref[...]
    gains[y, 0] = gm_ref[...]
    gains[y, 1] = go_ref[...]
    lat = lat_ref[...]
    k = jnp.dot(lat, wk_ref[...], preferred_element_type=F32)
    v = jnp.dot(lat, wv_ref[...], preferred_element_type=F32)
    cst, snt, rkt = cs_ref[...], sn_ref[...], rk_ref[...].astype(F32)
    swapped = jnp.concatenate([rkt[ROPE // 2 :], rkt[: ROPE // 2]], axis=0)
    krt = rkt * cst + swapped * snt
    table = jnp.transpose(jnp.concatenate([cst, snt, krt, krt], axis=0))
    kr = table[:, 2 * ROPE : 3 * ROPE]
    krp = jnp.concatenate([kr[TQ * i : TQ * i + TQ] for i in range(4)], axis=1).astype(BF)
    for h in range(4):
        kv = jnp.concatenate([k[:, HD * h : HD * h + HD], v[:, HD * h : HD * h + HD]], axis=1).astype(BF)
        for i in range(4):
            kvsend[h, i] = kv[TQ * i : TQ * i + TQ]
        kvsend[h, 4] = krp

    zdev = lambda p: dev(p, x, c, y)
    xdev = lambda p: dev(z, p, c, y)
    ydev = lambda p: dev(z, x, c, p)

    def pairs(ss, rs):
        return [(ss.at[d], rs.at[d]) for d in (0, 1)]

    ring_kv = Ring(
        NZ, z, zdev,
        lambda p: kvr.at[p, c],
        lambda p, h: kvr.at[p, c, :, rows48(mod4(x - h)), :],
        pairs(s_zkv, r_zkv), log,
        travel=tuple((d, h) for h in (0, 1, 3, 2) for d in (0, 1)),
        last=((0, 0), (1, 3), (0, 1), (1, 2)),
    )
    ring_gu = Ring(
        NZ, z, zdev,
        lambda p: wgu.at[:, p, x, c],
        lambda p, h: wgu.at[:, p, x, c, pl.ds(16 * h, 16), :],
        pairs(s_zgu, r_zgu), log,
    )
    ring_wd = Ring(
        NX, x, xdev,
        lambda p: wdt.at[z, p, c],
        lambda p, h: wdt.at[z, p, c, pl.ds(16 * h, 16), :],
        pairs(s_xwd, r_xwd), log,
    )
    ring_wdz = Ring(
        NZ, z, zdev,
        lambda p: wdt.at[p, :, c],
        lambda p, h: wdt.at[p, pl.ds(2 * h, 2), c],
        pairs(s_zwd, r_zwd), log,
    )
    ring_wo = Ring(
        NY, y, ydev,
        lambda p: wo.at[p, pl.ds(pl.multiple_of(128 * c, 128), 128), :],
        lambda p, h: wo.at[p, pl.ds(pl.multiple_of(128 * c + 64 * h, 64), 64), :],
        pairs(s_ywo, r_ywo), log,
    )
    ring_h = Ring(
        NY, y, ydev,
        lambda p: hid.at[p],
        lambda p, h: hid.at[p, :, pl.ds(1024 * h, 1024)],
        pairs(s_yh, r_yh), log,
        travel=((0, 0), (1, 1), (0, 1), (1, 0)),
    )

    def gu_ring(k):
        p = zk(k)
        return Ring(
            NX, x, xdev,
            lambda q: wgu.at[:, p, q, c],
            lambda q, h: wgu.at[:, p, q, c, pl.ds(16 * h, 16), :],
            [(s_xgu.at[k % NZ, d], r_xgu.at[k % NZ, d]) for d in (0, 1)], log,
        )

    xr = {k: gu_ring(k) for k in (0, -1, 1, -2, 2, -3, 3, 4)}

    def kv_out(k):
        to_partner(kvr.at[zk(k), c], s_dkv.at[k % NZ], r_dkv.at[k % NZ])

    def kv_in(k):
        come(kvr.at[zk(k), 1 - c], s_dkv.at[k % NZ], r_dkv.at[k % NZ])

    def gu_out(k):
        to_partner(wgu.at[:, zk(k), :, c], s_dgu.at[k % NZ], r_dgu.at[k % NZ])

    def gu_in(k):
        come(wgu.at[:, zk(k), :, 1 - c], s_dgu.at[k % NZ], r_dgu.at[k % NZ])

    def wd_out(k):
        to_partner(wdt.at[zk(k), :, c], s_dwd.at[k % NZ], r_dwd.at[k % NZ])

    def wd_in(k):
        come(wdt.at[zk(k), :, 1 - c], s_dwd.at[k % NZ], r_dwd.at[k % NZ])

    def wo_out(k):
        to_partner(ring_wo.blk(ring_wo.at(k)), s_dwo.at[k % NY - 1], r_dwo.at[k % NY - 1])

    def wo_in(k):
        ref = wo.at[ring_wo.at(k), pl.ds(pl.multiple_of(128 - 128 * c, 128), 128), :]
        come(ref, s_dwo.at[k % NY - 1], r_dwo.at[k % NY - 1])

    kvr[z, c, :, rows48(x), :] = kvsend[x]

    pl.semaphore_wait(barrier, len(peers))

    for d in (0, 1):
        ring_kv.send(z, d, 0, 0)
    for dx in (1, 3, 2):
        xt = mod4(x + dx)
        go(rcopy(kvsend.at[xt], kvr.at[z, c, :, rows48(x), :], s_kvx.at[dx - 1], r_kvx.at[dx - 1], xdev(xt)))
    ring_gu.start()
    cs, sn = table[:, :ROPE], table[:, ROPE : 2 * ROPE]
    q = q_ref[...].astype(F32)
    for h in range(4):
        qr = q[:, 96 * h + HD : 96 * h + 96]
        turned = qr * cs + jnp.concatenate([qr[:, ROPE // 2 :], qr[:, : ROPE // 2]], axis=1) * sn
        full = jnp.concatenate([q[:, 96 * h : 96 * h + HD], turned, jnp.zeros((T, 32), F32)], axis=1)
        qsend[h] = full.astype(BF)
    for dx in (1, 3, 2):
        xt = mod4(x + dx)
        go(rcopy(qsend.at[xt], qin.at[x], s_qx.at[dx - 1], r_qx.at[dx - 1], xdev(xt)))
    qin[x] = qsend[x]
    xr[0].start()
    ring_wd.start()

    for dy in (1, 3, 2):
        yt = mod4(y + dy)
        go(rcopy(res_ref.at[rows48(yt), :], resb.at[y], s_res.at[dy - 1], r_res.at[dy - 1], ydev(yt)))
        go(rcopy(gains.at[y], gains.at[y], s_g.at[dy - 1], r_g.at[dy - 1], ydev(yt)))
    resb[y] = res_ref[rows48(y), :]
    ring_wo.start()

    for dx in (1, 3, 2):
        come(kvr.at[z, c, :, rows48(mod4(x - dx)), :], s_kvx.at[dx - 1], r_kvx.at[dx - 1])
        for d in (0, 1):
            ring_kv.send(z, d, 0, dx)
    kv_out(0)

    kvt[...] = jnp.ones_like(kvt)
    obuf[...] = jnp.zeros_like(obuf)
    mbuf[...] = jnp.full_like(mbuf, -1e30)
    for dx in (1, 3, 2):
        come(qin.at[mod4(x - dx)], s_qx.at[dx - 1], r_qx.at[dx - 1])
    qt[...] = jnp.transpose(qin[...].reshape(NQ, 128))

    def attend(p):
        for cc in range(2):
            kr = kvr[p, cc, 4]
            for i in range(4):
                lo = (cc * 4 + i) * T
                kp[lo : lo + T] = jnp.concatenate(
                    [kvr[p, cc, i][:, :HD], kr[:, ROPE * i : ROPE * i + ROPE], jnp.zeros((T, ROPE), BF)], axis=1
                )
            kvt[cc, HD:128] = jnp.transpose(kvr[p, cc, 0:4].reshape(NQ, 128))[HD:128]

        def scores(qb, j):
            s = jnp.dot(kp[T * j : T * j + T], qt[:, QB * qb : QB * qb + QB], preferred_element_type=F32)
            sbuf[qb % 2, T * j : T * j + T] = s
            return jnp.max(s.reshape(T // 8, 8, QB), axis=0)

        maxima = [scores(0, j) for j in range(8)]
        for qb in range(3):
            qs = slice(QB * qb, QB * qb + QB)
            b = qb % 2
            top = maxima[0]
            for other in maxima[1:]:
                top = jnp.maximum(top, other)
            m_old = mbuf[0:1, qs]
            m_new = jnp.maximum(m_old, jnp.max(top, axis=0, keepdims=True))
            mbuf[0:1, qs] = m_new
            factor = jnp.exp2((m_old - m_new) * SCALE)
            shift = m_new * SCALE
            maxima = []
            acc = None
            for j in range(8):
                if qb < 2:
                    maxima.append(scores(qb + 1, j))
                pbuf[b, T * j : T * j + T] = jnp.exp2(sbuf[b, T * j : T * j + T] * SCALE - shift).astype(BF)
                if j % 4 == 3:
                    cc = j // 4
                    got = jnp.dot(kvt[cc], pbuf[b, cc * NQ : cc * NQ + NQ], preferred_element_type=F32)
                    acc = got if acc is None else acc + got
            obuf[:, qs] = obuf[:, qs] * factor + acc

    ring_gu.take(1)
    xr[-1].start()
    xr[1].start()
    kv_in(0)
    attend(z)
    ring_kv.step(1)
    kv_out(-1)
    kv_out(1)
    ring_wd.step(1)
    xr[0].step(1)
    kv_in(-1)
    attend(zk(-1))
    kv_in(1)
    attend(zk(1))
    ring_kv.step(2)
    kv_out(-2)
    kv_out(2)
    ring_wd.step(2)
    wd_out(0)
    xr[0].step(2)
    gu_out(0)
    xr[-1].step(1)
    xr[1].step(1)
    ring_wo.step(1)
    wo_out(-1)
    wo_out(1)
    kv_in(-2)
    attend(zk(-2))
    kv_in(2)
    attend(zk(2))
    ring_kv.step(3)
    kv_out(-3)
    kv_out(3)
    ring_gu.pass_on(1)
    xr[-1].step(2)
    gu_out(-1)
    xr[1].step(2)
    gu_out(1)
    kv_in(-3)
    attend(zk(-3))
    ring_kv.step(4)
    kv_out(4)
    ring_wo.step(2)
    wo_out(2)
    kv_in(3)
    attend(zk(3))
    ring_gu.step(2)
    xr[-2].start()
    xr[2].start()
    ring_wdz.start()
    kv_in(4)
    attend(zk(4))
    ring_gu.step(3)
    xr[-3].start()
    xr[3].start()

    par = lax.rem(x, 2).astype(F32)
    on = obuf[HD:128] / obuf[0:1]
    full = jnp.concatenate([on * (1.0 - par), on * par], axis=0)
    osend[...] = jnp.transpose(full).astype(BF).reshape(4, T, 128)
    others = [(dx, dy) for dx in range(4) for dy in range(4) if dx or dy]
    for dx, dy in sorted(others, key=lambda o: -(min(o[0], 4 - o[0]) + min(o[1], 4 - o[1]))):
        xt, yt = mod4(x + dx), mod4(y + dy)
        n = dx * 4 + dy - 1
        go(rcopy(osend.at[xt, rows48(yt), :], hb.at[4 * y + x], s_o.at[n], r_o.at[n], dev(z, xt, c, yt)))
    hb[4 * y + x] = osend[x, rows48(y), :]
    xr[-2].step(1)
    xr[2].step(1)
    ring_wdz.step(1)
    wd_out(-1)
    wd_out(1)
    for dy in (1, 3, 2):
        yf = mod4(y - dy)
        come(resb.at[yf], s_res.at[dy - 1], r_res.at[dy - 1])
        come(gains.at[yf], s_g.at[dy - 1], r_g.at[dy - 1])
    for kk in (-1, 1, 2):
        wo_in(kk)
    for dx, dy in others:
        n = dx * 4 + dy - 1
        come(hb.at[4 * mod4(y - dy) + mod4(x - dx)], s_o.at[n], r_o.at[n])

    attn = None
    for g in range(4):
        heads = [hb[4 * g + 2 * j] + hb[4 * g + 2 * j + 1] for j in range(2)]
        term = jnp.dot(jnp.concatenate(heads, axis=1), wo[g], preferred_element_type=F32)
        term = term.astype(BF).astype(F32)
        attn = term if attn is None else attn + term
    res = jnp.concatenate([resb[g] for g in range(4)], axis=1).astype(F32)
    rows = ALPHA * res + attn
    mean = jnp.sum(rows, axis=1, keepdims=True) * (1.0 / D)
    var = jnp.sum(rows * rows, axis=1, keepdims=True) * (1.0 / D) - mean * mean
    gain = jnp.concatenate([gains[g, 0] for g in range(4)], axis=1)
    hid[y] = ((rows - mean) * lax.rsqrt(var + EPS) * gain).astype(BF)

    ring_h.start()
    ring_gu.step(4)
    xr[4].start()
    xr[-2].step(2)
    gu_out(-2)
    xr[2].step(2)
    gu_out(2)
    xr[-3].step(1)
    xr[3].step(1)
    ring_wdz.step(2)
    wd_out(-2)
    wd_out(2)
    xr[-3].step(2)
    gu_out(-3)
    xr[3].step(2)
    gu_out(3)
    ring_h.step(1)
    xr[4].step(1)
    ring_wdz.step(3)
    wd_out(-3)
    wd_out(3)
    xr[4].step(2)
    gu_out(4)
    for kk in (0, -1, 1, -2, 2, -3, 3, 4):
        gu_in(kk)

    def gate_up(blocks, lo):
        rows = blocks[0] if len(blocks) == 1 else jnp.concatenate(blocks, axis=0)
        n = rows.shape[0]

        def one(j, carry):
            cols = pl.ds(pl.multiple_of(j * QB, QB), QB)
            gate = jnp.dot(rows, wgu[0, :, :, :, :, cols].reshape(D, QB), preferred_element_type=F32)
            up = jnp.dot(rows, wgu[1, :, :, :, :, cols].reshape(D, QB), preferred_element_type=F32)
            mixed[lo : lo + n, cols] = (gate / (1.0 + jnp.exp(-gate)) * up).astype(BF)
            return carry

        lax.fori_loop(0, FC // QB, one, 0)

    def down(slot, count):
        units = mixed[TQ * slot : TQ * (slot + count)]

        def one(j, carry):
            w = wdt[j].reshape(QB, FC)
            got = lax.dot_general(units, w, (((1,), (1,)), ((), ())), preferred_element_type=F32)
            got = got.astype(BF).reshape(count, TQ, QB)
            part[slot : slot + count, :, pl.ds(pl.multiple_of(j * QB, QB), QB)] = got
            return carry

        lax.fori_loop(0, NZ, one, 0)

    dist = (0, -1, 1, 2)

    def send_parts(slots):
        for s in slots:
            for dy in (2, 1, 3):
                yt = mod4(y + dy)
                dst = crec.at[dy - 1, mod4(y + dist[s])]
                go(rcopy(part.at[s, :, cols512(yt)], dst, s_p.at[dy - 1, s], r_p.at[dy - 1, s], ydev(yt)))

    gate_up([hid[y], hid[mod4(y - 1)], hid[mod4(y + 1)]], 0)
    ring_h.step(2)
    ring_wdz.step(4)
    wd_out(4)
    gate_up([hid[mod4(y + 2)]], 3 * TQ)
    for kk in (0, -1, 1, -2, 2, -3, 3, 4):
        wd_in(kk)
    down(0, 3)
    send_parts((0, 1, 2))
    down(3, 1)
    send_parts((3,))
    for s in range(4):
        crec[3, mod4(y + dist[s])] = part[s, :, cols512(y)]
    total = crec[3].astype(F32)
    for dy in (1, 3, 2):
        for s in range(4):
            come(crec.at[dy - 1, mod4(y - dy + dist[s])], s_p.at[dy - 1, s], r_p.at[dy - 1, s])
        total = total + crec[dy - 1].astype(F32)
    rows = (ALPHA * hid[:, :, cols512(y)].astype(F32) + HALF * total).reshape(T, 512)
    lane = lax.broadcasted_iota(jnp.int32, (T, 128), 1)
    s1 = jnp.sum(rows, axis=1, keepdims=True)
    s2 = jnp.sum(rows * rows, axis=1, keepdims=True)
    sums = jnp.where(lane == 0, s1, jnp.where(lane == 1, s2, 0.0))
    stat[0] = jnp.transpose(sums)[0:8]
    for dy in (2, 1, 3):
        go(rcopy(stat.at[0], stat.at[dy], s_f.at[dy - 1], r_f.at[dy - 1], ydev(mod4(y + dy))))
    both = stat[0]
    for dy in (1, 3, 2):
        come(stat.at[dy], s_f.at[dy - 1], r_f.at[dy - 1])
        both = both + stat[dy]
    both = jnp.transpose(jnp.concatenate([both, jnp.zeros((120, T), F32)], axis=0))
    mean = both[:, 0:1] * (1.0 / D)
    var = both[:, 1:2] * (1.0 / D) - mean * mean
    out_ref[...] = ((rows - mean) * lax.rsqrt(var + EPS) * gains[y, 1]).astype(BF)
    for cp in log:
        cp.wait_send()


def local(queries, latents, rope_key, w_key, w_value, w_out, resid, gain_mix, w_gate, w_up, w_down, gain_out):
    start = lax.axis_index("sp") * T
    positions = start + jnp.arange(T, dtype=jnp.int32)
    grid_rows = (positions // GRID_W).astype(F32)
    grid_cols = (positions % GRID_W).astype(F32)
    count = ROPE // 4
    inverse = ROTARY_BASE ** (-jnp.arange(count, dtype=F32) / count)
    angles = jnp.concatenate([inverse[:, None] * grid_rows, inverse[:, None] * grid_cols], axis=0)
    cos, sin = jnp.cos(angles), jnp.sin(angles)
    cs = jnp.concatenate([cos, cos], axis=0)
    sn = jnp.concatenate([-sin, sin], axis=0)
    dma = pltpu.SemaphoreType.DMA
    V = pltpu.VMEM

    def pair(*shape):
        return [dma(shape), dma(shape)]

    sems = []
    for shape in (
        (3,), (3,), (3,), (3,),
        (2, 4, 4), (8,), (2, 4), (8, 2, 2), (8,),
        (2, 2), (2, 4), (8,), (2, 2), (3,),
        (15,), (2, 2, 2), (3, 4), (3,),
    ):
        sems += pair(*shape)
    scratch = [
        V((4, 5, TQ, 128), BF),
        V((4, T, 128), BF),
        V((NZ, 2, 5, T, 128), BF),
        V((4, T, 128), BF),
        V((128, NQ), BF),
        V((8 * T, 128), BF),
        V((2, 128, NQ), BF),
        V((2, 8 * T, QB), F32),
        V((2, 8 * T, QB), BF),
        V((128, NQ), F32),
        V((8, NQ), F32),
        V((4, T, 128), BF),
        V((16, TQ, 128), BF),
        V((NY, 256, D), BF),
        V((NY, TQ, 512), BF),
        V((NY, 2, 1, 512), F32),
        V((2, NZ, NX, 2, 32, FC), BF),
        V((NZ, NX, 2, 32, FC), BF),
        V((NY, TQ, D), BF),
        V((T, FC), BF),
        V((NY, TQ, D), BF),
        V((NY, NY, TQ, 512), BF),
        V((NY, 8, T), F32),
    ]
    vm = pl.BlockSpec(memory_space=pltpu.VMEM)
    return pl.pallas_call(
        kernel,
        out_shape=jax.ShapeDtypeStruct((T, 512), BF),
        in_specs=[vm] * 14,
        out_specs=vm,
        scratch_shapes=scratch + sems,
        compiler_params=pltpu.CompilerParams(
            collective_id=0, has_side_effects=True, vmem_limit_bytes=60 * 1024 * 1024
        ),
    )(
        queries, latents, rope_key.T, w_key, w_value, w_out, resid, gain_mix.reshape(1, 512),
        w_gate, w_up, w_down.T, gain_out.reshape(1, 512), cs, sn,
    )


def solution(mesh):
    placed = (
        P("sp", "tp"), P("sp", None), P("sp", None), P(None, "tp"), P(None, "tp"), P("tp", None),
        P("sp", "tp"), P("tp"), P("sp", "tp"), P("sp", "tp"), P("tp", "sp"), P("tp"),
    )
    return jax.shard_map(local, mesh=mesh, in_specs=placed, out_specs=P("sp", "tp"), check_vma=False)
```

```python
import jax
import jax.numpy as jnp
from jax import lax
from jax.experimental import pallas as pl
from jax.experimental.pallas import tpu as pltpu
from jax.sharding import PartitionSpec as P

MESH = pl.DeviceIdType.MESH
F32 = jnp.float32
BF = jnp.bfloat16

HD = 64
ROPE = 32
GRID_W = 64
ROTARY_BASE = 10000.0
EPS = 1e-06
ALPHA = 8.0**0.25
HALF = 0.5
NZ, NX, NY = 8, 4, 4
T = 192
TQ = 48
NQ = 768
QB = 256
D = 2048
FC = 768
SCALE = (1.4426950408889634) * (96.0**-0.5)


class Ring:
    WHOLE = ((0, None), (1, None))
    HALVES = ((0, 0), (1, 1))

    def __init__(self, n, pos, dev, blk, half, sems, log, travel=WHOLE, last=HALVES):
        self.n, self.pos, self.dev, self.travel, self.last = n, pos, dev, travel, last
        self.blk, self.half, self.sems, self.log = blk, half, sems, log
        self.pieces = travel is not self.WHOLE

    def at(self, k):
        return lax.rem(self.pos + (k + 2 * self.n), self.n)

    def copy(self, p, d, t, h):
        ss, rs = self.sems[d]
        ref = self.blk(p) if h is None else self.half(p, h)
        at = (t, h) if self.pieces else (t,)
        return pltpu.make_async_remote_copy(
            src_ref=ref,
            dst_ref=ref,
            send_sem=ss.at[at],
            recv_sem=rs.at[at],
            device_id=self.dev(self.at(1 if d == 0 else -1)),
            device_id_type=MESH,
        )

    def parts(self, t):
        return self.last if t == self.n // 2 - 1 else self.travel

    def send(self, p, d, t, h):
        cp = self.copy(p, d, t, h)
        cp.start()
        self.log.append(cp)

    def start(self):
        for d, h in self.parts(0):
            self.send(self.pos, d, 0, h)

    def arrived(self, d, t):
        return self.at(-t if d == 0 else t)

    def take(self, t):
        for d, h in self.parts(t - 1):
            self.copy(self.arrived(d, t), d, t - 1, h).wait_recv()

    def pass_on(self, t):
        for d, h in self.parts(t):
            self.send(self.arrived(d, t), d, t, h)

    def step(self, t):
        for d, h in self.parts(t - 1):
            p = self.arrived(d, t)
            self.copy(p, d, t - 1, h).wait_recv()
            if self.pieces and t < self.n // 2 and (d, h) in self.parts(t):
                self.send(p, d, t, h)
        if not self.pieces and t < self.n // 2:
            self.pass_on(t)


def kernel(
    q_ref, lat_ref, rk_ref, wk_ref, wv_ref, wo_ref, res_ref, gm_ref, wg_ref, wu_ref, wd_ref, go_ref, cs_ref, sn_ref,
    out_ref,
    kvsend, qsend, kvr, qin, qt, kp, kvt, sbuf, pbuf, obuf, mbuf, osend, hb, wo, resb, gains,
    w3, hid, mixed, part, crec, acc, stat,
    s_kvx, r_kvx, s_qx, r_qx, s_res, r_res, s_g, r_g,
    s_zkv, r_zkv, s_dkv, r_dkv, s_zw, r_zw, s_xw, r_xw, s_dw, r_dw, s_ywo, r_ywo, s_dwo, r_dwo,
    s_o, r_o, s_yh, r_yh, s_p, r_p, s_f, r_f,
):
    sp = lax.axis_index("sp")
    y = lax.axis_index("tp")
    c = lax.rem(sp, 2)
    x = lax.rem(sp // 2, NX)
    z = sp // (2 * NX)
    log = []

    def dev(zz, xx, cc, yy):
        return ((zz * NX + xx) * 2 + cc, yy)

    def mod4(v):
        return lax.rem(v + 8, 4)

    def zk(k):
        return lax.rem(z + k + NZ, NZ)

    partner = dev(z, x, 1 - c, y)

    def rcopy(src, dst, ss, rs, to):
        return pltpu.make_async_remote_copy(
            src_ref=src, dst_ref=dst, send_sem=ss, recv_sem=rs, device_id=to, device_id_type=MESH
        )

    def go(cp):
        cp.start()
        log.append(cp)

    def come(ref, ss, rs):
        rcopy(ref, ref, ss, rs, partner).wait_recv()

    def to_partner(ref, ss, rs):
        go(rcopy(ref, ref, ss, rs, partner))

    def rows48(i):
        return pl.ds(pl.multiple_of(TQ * i, 16), TQ)

    def cols512(i):
        return pl.ds(pl.multiple_of(512 * i, 512), 512)

    barrier = pltpu.get_barrier_semaphore()
    peers = [dev(z, mod4(x + dx), c, mod4(y + dy)) for dx in range(4) for dy in range(4) if dx or dy]
    peers += [dev(zk(1), x, c, y), dev(zk(-1), x, c, y), partner]
    for peer in peers:
        pl.semaphore_signal(barrier, inc=1, device_id=peer, device_id_type=MESH)

    w3[0, z, x, c] = wg_ref[...]
    w3[1, z, x, c] = wu_ref[...]
    w3[2, z, x, c] = wd_ref[...]
    wo[y] = wo_ref[...]
    gains[y, 0] = gm_ref[...]
    gains[y, 1] = go_ref[...]
    lat = lat_ref[...]
    k = jnp.dot(lat, wk_ref[...], preferred_element_type=F32)
    v = jnp.dot(lat, wv_ref[...], preferred_element_type=F32)
    cst, snt, rkt = cs_ref[...], sn_ref[...], rk_ref[...].astype(F32)
    swapped = jnp.concatenate([rkt[ROPE // 2 :], rkt[: ROPE // 2]], axis=0)
    krt = rkt * cst + swapped * snt
    table = jnp.transpose(jnp.concatenate([cst, snt, krt, krt], axis=0))
    kr = table[:, 2 * ROPE : 3 * ROPE]
    krp = jnp.concatenate([kr[TQ * i : TQ * i + TQ] for i in range(4)], axis=1).astype(BF)
    for h in range(4):
        kv = jnp.concatenate([k[:, HD * h : HD * h + HD], v[:, HD * h : HD * h + HD]], axis=1).astype(BF)
        for i in range(4):
            kvsend[h, i] = kv[TQ * i : TQ * i + TQ]
        kvsend[h, 4] = krp

    zdev = lambda p: dev(p, x, c, y)
    xdev = lambda p: dev(z, p, c, y)
    ydev = lambda p: dev(z, x, c, p)

    def pairs(ss, rs):
        return [(ss.at[d], rs.at[d]) for d in (0, 1)]

    ring_kv = Ring(
        NZ, z, zdev,
        lambda p: kvr.at[p, c],
        lambda p, h: kvr.at[p, c, :, rows48(mod4(x - h)), :],
        pairs(s_zkv, r_zkv), log,
        travel=tuple((d, h) for h in (0, 1, 3, 2) for d in (0, 1)),
        last=((0, 0), (1, 3), (0, 1), (1, 2)),
    )
    ring_w = Ring(
        NZ, z, zdev,
        lambda p: w3.at[:, p, x, c],
        lambda p, h: w3.at[:, p, x, c, pl.ds(16 * h, 16), :],
        pairs(s_zw, r_zw), log,
    )
    ring_wo = Ring(
        NY, y, ydev,
        lambda p: wo.at[p, pl.ds(pl.multiple_of(128 * c, 128), 128), :],
        lambda p, h: wo.at[p, pl.ds(pl.multiple_of(128 * c + 64 * h, 64), 64), :],
        pairs(s_ywo, r_ywo), log,
    )
    ring_h = Ring(
        NY, y, ydev,
        lambda p: hid.at[p],
        lambda p, h: hid.at[p, :, pl.ds(1024 * h, 1024)],
        pairs(s_yh, r_yh), log,
        travel=((0, 0), (1, 1), (0, 1), (1, 0)),
    )

    def x_ring(k):
        p = zk(k)
        return Ring(
            NX, x, xdev,
            lambda q: w3.at[:, p, q, c],
            lambda q, h: w3.at[:, p, q, c, pl.ds(16 * h, 16), :],
            [(s_xw.at[k % NZ, d], r_xw.at[k % NZ, d]) for d in (0, 1)], log,
        )

    xr = {k: x_ring(k) for k in (0, -1, 1, -2, 2, -3, 3, 4)}

    def kv_out(k):
        to_partner(kvr.at[zk(k), c], s_dkv.at[k % NZ], r_dkv.at[k % NZ])

    def kv_in(k):
        come(kvr.at[zk(k), 1 - c], s_dkv.at[k % NZ], r_dkv.at[k % NZ])

    def w_out(k):
        to_partner(w3.at[:, zk(k), :, c], s_dw.at[k % NZ], r_dw.at[k % NZ])

    def w_in(k):
        come(w3.at[:, zk(k), :, 1 - c], s_dw.at[k % NZ], r_dw.at[k % NZ])

    def wo_out(k):
        to_partner(ring_wo.blk(ring_wo.at(k)), s_dwo.at[k % NY - 1], r_dwo.at[k % NY - 1])

    def wo_in(k):
        ref = wo.at[ring_wo.at(k), pl.ds(pl.multiple_of(128 - 128 * c, 128), 128), :]
        come(ref, s_dwo.at[k % NY - 1], r_dwo.at[k % NY - 1])

    kvr[z, c, :, rows48(x), :] = kvsend[x]

    cs, sn = table[:, :ROPE], table[:, ROPE : 2 * ROPE]
    q = q_ref[...].astype(F32)
    for h in range(4):
        qr = q[:, 96 * h + HD : 96 * h + 96]
        turned = qr * cs + jnp.concatenate([qr[:, ROPE // 2 :], qr[:, : ROPE // 2]], axis=1) * sn
        full = jnp.concatenate([q[:, 96 * h : 96 * h + HD], turned, jnp.zeros((T, 32), F32)], axis=1)
        qsend[h] = full.astype(BF)
    qin[x] = qsend[x]
    resb[y] = res_ref[rows48(y), :]
    kvt[...] = jnp.ones_like(kvt)
    obuf[...] = jnp.zeros_like(obuf)
    mbuf[...] = jnp.full_like(mbuf, -1e30)

    pl.semaphore_wait(barrier, len(peers))

    for d in (0, 1):
        ring_kv.send(z, d, 0, 0)
    for dx in (1, 3, 2):
        xt = mod4(x + dx)
        go(rcopy(kvsend.at[xt], kvr.at[z, c, :, rows48(x), :], s_kvx.at[dx - 1], r_kvx.at[dx - 1], xdev(xt)))
    ring_w.start()
    for dx in (1, 3, 2):
        xt = mod4(x + dx)
        go(rcopy(qsend.at[xt], qin.at[x], s_qx.at[dx - 1], r_qx.at[dx - 1], xdev(xt)))
    xr[0].start()

    for dy in (1, 3, 2):
        yt = mod4(y + dy)
        go(rcopy(res_ref.at[rows48(yt), :], resb.at[y], s_res.at[dy - 1], r_res.at[dy - 1], ydev(yt)))
        go(rcopy(gains.at[y], gains.at[y], s_g.at[dy - 1], r_g.at[dy - 1], ydev(yt)))
    ring_wo.start()

    for dx in (1, 3, 2):
        come(kvr.at[z, c, :, rows48(mod4(x - dx)), :], s_kvx.at[dx - 1], r_kvx.at[dx - 1])
        for d in (0, 1):
            ring_kv.send(z, d, 0, dx)
    kv_out(0)

    for dx in (1, 3, 2):
        come(qin.at[mod4(x - dx)], s_qx.at[dx - 1], r_qx.at[dx - 1])
    qt[...] = jnp.transpose(qin[...].reshape(NQ, 128))

    def attend(p):
        for cc in range(2):
            kr = kvr[p, cc, 4]
            for i in range(4):
                lo = (cc * 4 + i) * T
                kp[lo : lo + T] = jnp.concatenate(
                    [kvr[p, cc, i][:, :HD], kr[:, ROPE * i : ROPE * i + ROPE], jnp.zeros((T, ROPE), BF)], axis=1
                )
            kvt[cc, HD:128] = jnp.transpose(kvr[p, cc, 0:4].reshape(NQ, 128))[HD:128]

        def scores(qb, j):
            s = jnp.dot(kp[T * j : T * j + T], qt[:, QB * qb : QB * qb + QB], preferred_element_type=F32)
            sbuf[qb % 2, T * j : T * j + T] = s
            return jnp.max(s.reshape(T // 8, 8, QB), axis=0)

        maxima = [scores(0, j) for j in range(8)]
        for qb in range(3):
            qs = slice(QB * qb, QB * qb + QB)
            b = qb % 2
            top = maxima[0]
            for other in maxima[1:]:
                top = jnp.maximum(top, other)
            m_old = mbuf[0:1, qs]
            m_new = jnp.maximum(m_old, jnp.max(top, axis=0, keepdims=True))
            mbuf[0:1, qs] = m_new
            factor = jnp.exp2((m_old - m_new) * SCALE)
            shift = m_new * SCALE
            maxima = []
            acc = None
            for j in range(8):
                if qb < 2:
                    maxima.append(scores(qb + 1, j))
                pbuf[b, T * j : T * j + T] = jnp.exp2(sbuf[b, T * j : T * j + T] * SCALE - shift).astype(BF)
                if j % 4 == 3:
                    cc = j // 4
                    got = jnp.dot(kvt[cc], pbuf[b, cc * NQ : cc * NQ + NQ], preferred_element_type=F32)
                    acc = got if acc is None else acc + got
            obuf[:, qs] = obuf[:, qs] * factor + acc

    ring_w.take(1)
    xr[-1].start()
    xr[1].start()
    kv_in(0)
    attend(z)
    ring_kv.step(1)
    kv_out(-1)
    kv_out(1)
    ring_w.pass_on(1)
    xr[0].step(1)
    kv_in(-1)
    attend(zk(-1))
    kv_in(1)
    attend(zk(1))
    ring_kv.step(2)
    kv_out(-2)
    kv_out(2)
    xr[0].step(2)
    w_out(0)
    xr[-1].step(1)
    xr[1].step(1)
    kv_in(-2)
    attend(zk(-2))
    kv_in(2)
    attend(zk(2))
    ring_w.take(2)
    xr[-2].start()
    xr[2].start()
    ring_kv.step(3)
    kv_out(-3)
    kv_out(3)
    ring_w.pass_on(2)
    xr[-1].step(2)
    w_out(-1)
    xr[1].step(2)
    w_out(1)
    ring_wo.step(1)
    wo_out(-1)
    wo_out(1)
    kv_in(-3)
    attend(zk(-3))
    ring_kv.step(4)
    kv_out(4)
    ring_wo.step(2)
    wo_out(2)
    kv_in(3)
    attend(zk(3))
    xr[-2].step(1)
    xr[2].step(1)
    kv_in(4)
    attend(zk(4))
    ring_w.step(3)
    xr[-3].start()
    xr[3].start()

    par = lax.rem(x, 2).astype(F32)
    on = obuf[HD:128] / obuf[0:1]
    full = jnp.concatenate([on * (1.0 - par), on * par], axis=0)
    osend[...] = jnp.transpose(full).astype(BF).reshape(4, T, 128)
    others = [(dx, dy) for dx in range(4) for dy in range(4) if dx or dy]
    for dx, dy in sorted(others, key=lambda o: -(min(o[0], 4 - o[0]) + min(o[1], 4 - o[1]))):
        xt, yt = mod4(x + dx), mod4(y + dy)
        n = dx * 4 + dy - 1
        go(rcopy(osend.at[xt, rows48(yt), :], hb.at[4 * y + x], s_o.at[n], r_o.at[n], dev(z, xt, c, yt)))
    hb[4 * y + x] = osend[x, rows48(y), :]
    xr[-2].step(2)
    w_out(-2)
    xr[2].step(2)
    w_out(2)
    ring_w.step(4)
    xr[4].start()
    for dy in (1, 3, 2):
        yf = mod4(y - dy)
        come(resb.at[yf], s_res.at[dy - 1], r_res.at[dy - 1])
        come(gains.at[yf], s_g.at[dy - 1], r_g.at[dy - 1])
    for kk in (-1, 1, 2):
        wo_in(kk)
    for dx, dy in others:
        n = dx * 4 + dy - 1
        come(hb.at[4 * mod4(y - dy) + mod4(x - dx)], s_o.at[n], r_o.at[n])

    attn = None
    for g in range(4):
        heads = [hb[4 * g + 2 * j] + hb[4 * g + 2 * j + 1] for j in range(2)]
        term = jnp.dot(jnp.concatenate(heads, axis=1), wo[g], preferred_element_type=F32)
        term = term.astype(BF).astype(F32)
        attn = term if attn is None else attn + term
    res = jnp.concatenate([resb[g] for g in range(4)], axis=1).astype(F32)
    rows = ALPHA * res + attn
    mean = jnp.sum(rows, axis=1, keepdims=True) * (1.0 / D)
    var = jnp.sum(rows * rows, axis=1, keepdims=True) * (1.0 / D) - mean * mean
    gain = jnp.concatenate([gains[g, 0] for g in range(4)], axis=1)
    hid[y] = ((rows - mean) * lax.rsqrt(var + EPS) * gain).astype(BF)

    ring_h.start()
    xr[-3].step(1)
    xr[3].step(1)
    xr[4].step(1)
    ring_h.step(1)
    xr[-3].step(2)
    w_out(-3)
    xr[3].step(2)
    w_out(3)
    xr[4].step(2)
    w_out(4)
    for kk in (0, -1, 1, -2, 2, -3, 3, 4):
        w_in(kk)

    def gate_up(blocks, lo):
        rows = blocks[0] if len(blocks) == 1 else jnp.concatenate(blocks, axis=0)
        n = rows.shape[0]

        def one(j, carry):
            cols = pl.ds(pl.multiple_of(j * QB, QB), QB)
            gate = jnp.dot(rows, w3[0, :, :, :, :, cols].reshape(D, QB), preferred_element_type=F32)
            up = jnp.dot(rows, w3[1, :, :, :, :, cols].reshape(D, QB), preferred_element_type=F32)
            mixed[lo : lo + n, cols] = (gate / (1.0 + jnp.exp(-gate)) * up).astype(BF)
            return carry

        lax.fori_loop(0, FC // QB, one, 0)

    dist = (0, -1, 1, 2)

    def down(slot, count):
        units = mixed[TQ * slot : TQ * (slot + count)]
        slots = slice(slot, slot + count)
        for dy in (2, 1, 3, 0):
            yt = mod4(y + dy)
            w = w3[2, pl.ds(2 * yt, 2)].reshape(512, FC)
            got = lax.dot_general(units, w, (((1,), (1,)), ((), ())), preferred_element_type=F32)
            got = got.astype(BF).reshape(count, TQ, 512)
            if dy:
                n = min(slot, 1)
                part[dy - 1, slots] = got
                src = part.at[dy - 1, pl.ds(slot, count)]
                dst = crec.at[dy - 1, pl.ds(slot, count)]
                go(rcopy(src, dst, s_p.at[dy - 1, n], r_p.at[dy - 1, n], ydev(yt)))
            else:
                for s in range(count):
                    acc[mod4(y + dist[slot + s])] = got[s].astype(F32)

    gate_up([hid[y], hid[mod4(y - 1)], hid[mod4(y + 1)]], 0)
    down(0, 3)
    ring_h.step(2)
    gate_up([hid[mod4(y + 2)]], 3 * TQ)
    down(3, 1)
    for n, slots in ((0, (0, 1, 2)), (1, (3,))):
        for dy in (1, 3, 2):
            come(crec.at[dy - 1, pl.ds(slots[0], len(slots))], s_p.at[dy - 1, n], r_p.at[dy - 1, n])
            for s in slots:
                b = mod4(y - dy + dist[s])
                acc[b] = acc[b] + crec[dy - 1, s].astype(F32)
    total = acc[...]
    rows = (ALPHA * hid[:, :, cols512(y)].astype(F32) + HALF * total).reshape(T, 512)
    lane = lax.broadcasted_iota(jnp.int32, (T, 128), 1)
    s1 = jnp.sum(rows, axis=1, keepdims=True)
    s2 = jnp.sum(rows * rows, axis=1, keepdims=True)
    sums = jnp.where(lane == 0, s1, jnp.where(lane == 1, s2, 0.0))
    stat[0] = jnp.transpose(sums)[0:8]
    for dy in (2, 1, 3):
        go(rcopy(stat.at[0], stat.at[dy], s_f.at[dy - 1], r_f.at[dy - 1], ydev(mod4(y + dy))))
    both = stat[0]
    for dy in (1, 3, 2):
        come(stat.at[dy], s_f.at[dy - 1], r_f.at[dy - 1])
        both = both + stat[dy]
    both = jnp.transpose(jnp.concatenate([both, jnp.zeros((120, T), F32)], axis=0))
    mean = both[:, 0:1] * (1.0 / D)
    var = both[:, 1:2] * (1.0 / D) - mean * mean
    out_ref[...] = ((rows - mean) * lax.rsqrt(var + EPS) * gains[y, 1]).astype(BF)
    for cp in log:
        cp.wait_send()


def local(queries, latents, rope_key, w_key, w_value, w_out, resid, gain_mix, w_gate, w_up, w_down, gain_out):
    start = lax.axis_index("sp") * T
    positions = start + jnp.arange(T, dtype=jnp.int32)
    grid_rows = (positions // GRID_W).astype(F32)
    grid_cols = (positions % GRID_W).astype(F32)
    count = ROPE // 4
    inverse = ROTARY_BASE ** (-jnp.arange(count, dtype=F32) / count)
    angles = jnp.concatenate([inverse[:, None] * grid_rows, inverse[:, None] * grid_cols], axis=0)
    cos, sin = jnp.cos(angles), jnp.sin(angles)
    cs = jnp.concatenate([cos, cos], axis=0)
    sn = jnp.concatenate([-sin, sin], axis=0)
    dma = pltpu.SemaphoreType.DMA
    V = pltpu.VMEM

    def pair(*shape):
        return [dma(shape), dma(shape)]

    sems = []
    for shape in (
        (3,), (3,), (3,), (3,),
        (2, 4, 4), (8,), (2, 4), (8, 2, 2), (8,),
        (2, 2), (3,),
        (15,), (2, 2, 2), (3, 2), (3,),
    ):
        sems += pair(*shape)
    scratch = [
        V((4, 5, TQ, 128), BF),
        V((4, T, 128), BF),
        V((NZ, 2, 5, T, 128), BF),
        V((4, T, 128), BF),
        V((128, NQ), BF),
        V((8 * T, 128), BF),
        V((2, 128, NQ), BF),
        V((2, 8 * T, QB), F32),
        V((2, 8 * T, QB), BF),
        V((128, NQ), F32),
        V((8, NQ), F32),
        V((4, T, 128), BF),
        V((16, TQ, 128), BF),
        V((NY, 256, D), BF),
        V((NY, TQ, 512), BF),
        V((NY, 2, 1, 512), F32),
        V((3, NZ, NX, 2, 32, FC), BF),
        V((NY, TQ, D), BF),
        V((T, FC), BF),
        V((3, NY, TQ, 512), BF),
        V((3, NY, TQ, 512), BF),
        V((NY, TQ, 512), F32),
        V((NY, 8, T), F32),
    ]
    vm = pl.BlockSpec(memory_space=pltpu.VMEM)
    return pl.pallas_call(
        kernel,
        out_shape=jax.ShapeDtypeStruct((T, 512), BF),
        in_specs=[vm] * 14,
        out_specs=vm,
        scratch_shapes=scratch + sems,
        compiler_params=pltpu.CompilerParams(
            collective_id=0, has_side_effects=True, vmem_limit_bytes=60 * 1024 * 1024
        ),
    )(
        queries, latents, rope_key.T, w_key, w_value, w_out, resid, gain_mix.reshape(1, 512),
        w_gate, w_up, w_down.T, gain_out.reshape(1, 512), cs, sn,
    )


def solution(mesh):
    placed = (
        P("sp", "tp"), P("sp", None), P("sp", None), P(None, "tp"), P(None, "tp"), P("tp", None),
        P("sp", "tp"), P("tp"), P("sp", "tp"), P("sp", "tp"), P("tp", "sp"), P("tp"),
    )
    return jax.shard_map(local, mesh=mesh, in_specs=placed, out_specs=P("sp", "tp"), check_vma=False)
```

```python
import jax
import jax.numpy as jnp
from jax import lax
from jax.experimental import pallas as pl
from jax.experimental.pallas import tpu as pltpu
from jax.sharding import PartitionSpec as P

MESH = pl.DeviceIdType.MESH
F32 = jnp.float32
BF = jnp.bfloat16

HD = 64
ROPE = 32
GRID_W = 64
ROTARY_BASE = 10000.0
EPS = 1e-06
ALPHA = 8.0**0.25
HALF = 0.5
NZ, NX, NY = 8, 4, 4
T = 192
TQ = 48
NQ = 768
QB = 256
D = 2048
FC = 768
SCALE = (1.4426950408889634) * (96.0**-0.5)


class Ring:
    WHOLE = ((0, None), (1, None))
    HALVES = ((0, 0), (1, 1))

    def __init__(self, n, pos, dev, blk, half, sems, log, travel=WHOLE, last=HALVES):
        self.n, self.pos, self.dev, self.travel, self.last = n, pos, dev, travel, last
        self.blk, self.half, self.sems, self.log = blk, half, sems, log
        self.pieces = travel is not self.WHOLE

    def at(self, k):
        return lax.rem(self.pos + (k + 2 * self.n), self.n)

    def copy(self, p, d, t, h):
        ss, rs = self.sems[d]
        ref = self.blk(p) if h is None else self.half(p, h)
        at = (t, h) if self.pieces else (t,)
        return pltpu.make_async_remote_copy(
            src_ref=ref,
            dst_ref=ref,
            send_sem=ss.at[at],
            recv_sem=rs.at[at],
            device_id=self.dev(self.at(1 if d == 0 else -1)),
            device_id_type=MESH,
        )

    def parts(self, t):
        return self.last if t == self.n // 2 - 1 else self.travel

    def send(self, p, d, t, h):
        cp = self.copy(p, d, t, h)
        cp.start()
        self.log.append(cp)

    def start(self):
        for d, h in self.parts(0):
            self.send(self.pos, d, 0, h)

    def arrived(self, d, t):
        return self.at(-t if d == 0 else t)

    def take(self, t):
        for d, h in self.parts(t - 1):
            self.copy(self.arrived(d, t), d, t - 1, h).wait_recv()

    def pass_on(self, t):
        for d, h in self.parts(t):
            self.send(self.arrived(d, t), d, t, h)

    def step(self, t):
        for d, h in self.parts(t - 1):
            p = self.arrived(d, t)
            self.copy(p, d, t - 1, h).wait_recv()
            if self.pieces and t < self.n // 2 and (d, h) in self.parts(t):
                self.send(p, d, t, h)
        if not self.pieces and t < self.n // 2:
            self.pass_on(t)


def kernel(
    q_ref, lat_ref, rk_ref, wk_ref, wv_ref, wo_ref, res_ref, gm_ref, wg_ref, wu_ref, wd_ref, go_ref, cs_ref, sn_ref,
    out_ref,
    kvsend, qsend, kvr, qin, qt, kp, kvt, sbuf, pbuf, obuf, mbuf, osend, hb, wo, resb, gains,
    w3, hid, mixed, part, crec, acc, stat,
    s_kvx, r_kvx, s_qx, r_qx, s_res, r_res, s_g, r_g,
    s_zkv, r_zkv, s_dkv, r_dkv, s_zw, r_zw, s_xw, r_xw, s_dw, r_dw, s_ywo, r_ywo, s_dwo, r_dwo,
    s_o, r_o, s_yh, r_yh, s_p, r_p, s_f, r_f,
):
    sp = lax.axis_index("sp")
    y = lax.axis_index("tp")
    c = lax.rem(sp, 2)
    x = lax.rem(sp // 2, NX)
    z = sp // (2 * NX)
    log = []

    def dev(zz, xx, cc, yy):
        return ((zz * NX + xx) * 2 + cc, yy)

    def mod4(v):
        return lax.rem(v + 8, 4)

    def zk(k):
        return lax.rem(z + k + NZ, NZ)

    partner = dev(z, x, 1 - c, y)

    def rcopy(src, dst, ss, rs, to):
        return pltpu.make_async_remote_copy(
            src_ref=src, dst_ref=dst, send_sem=ss, recv_sem=rs, device_id=to, device_id_type=MESH
        )

    def go(cp):
        cp.start()
        log.append(cp)

    def come(ref, ss, rs):
        rcopy(ref, ref, ss, rs, partner).wait_recv()

    def to_partner(ref, ss, rs):
        go(rcopy(ref, ref, ss, rs, partner))

    def rows48(i):
        return pl.ds(pl.multiple_of(TQ * i, 16), TQ)

    def cols512(i):
        return pl.ds(pl.multiple_of(512 * i, 512), 512)

    barrier = pltpu.get_barrier_semaphore()
    peers = [dev(z, mod4(x + dx), c, mod4(y + dy)) for dx in range(4) for dy in range(4) if dx or dy]
    peers += [dev(zk(1), x, c, y), dev(zk(-1), x, c, y), partner]
    for peer in peers:
        pl.semaphore_signal(barrier, inc=1, device_id=peer, device_id_type=MESH)

    w3[0, z, x, c] = wg_ref[...]
    w3[1, z, x, c] = wu_ref[...]
    w3[2, z, x, c] = wd_ref[...]
    wo[y] = wo_ref[...]
    gains[y, 0] = gm_ref[...]
    gains[y, 1] = go_ref[...]
    lat = lat_ref[...]
    k = jnp.dot(lat, wk_ref[...], preferred_element_type=F32)
    v = jnp.dot(lat, wv_ref[...], preferred_element_type=F32)
    cst, snt, rkt = cs_ref[...], sn_ref[...], rk_ref[...].astype(F32)
    swapped = jnp.concatenate([rkt[ROPE // 2 :], rkt[: ROPE // 2]], axis=0)
    krt = rkt * cst + swapped * snt
    table = jnp.transpose(jnp.concatenate([cst, snt, krt, krt], axis=0))
    kr = table[:, 2 * ROPE : 3 * ROPE]
    krp = jnp.concatenate([kr[TQ * i : TQ * i + TQ] for i in range(4)], axis=1).astype(BF)
    for h in range(4):
        kv = jnp.concatenate([k[:, HD * h : HD * h + HD], v[:, HD * h : HD * h + HD]], axis=1).astype(BF)
        for i in range(4):
            kvsend[h, i] = kv[TQ * i : TQ * i + TQ]
        kvsend[h, 4] = krp

    zdev = lambda p: dev(p, x, c, y)
    xdev = lambda p: dev(z, p, c, y)
    ydev = lambda p: dev(z, x, c, p)

    def pairs(ss, rs):
        return [(ss.at[d], rs.at[d]) for d in (0, 1)]

    ring_kv = Ring(
        NZ, z, zdev,
        lambda p: kvr.at[p, c],
        lambda p, h: kvr.at[p, c, :, rows48(mod4(x - h)), :],
        pairs(s_zkv, r_zkv), log,
        travel=tuple((d, h) for h in (0, 1, 3, 2) for d in (0, 1)),
        last=((0, 0), (1, 3), (0, 1), (1, 2)),
    )
    ring_w = Ring(
        NZ, z, zdev,
        lambda p: w3.at[:, p, x, c],
        lambda p, h: w3.at[:, p, x, c, pl.ds(16 * h, 16), :],
        pairs(s_zw, r_zw), log,
    )
    ring_wo = Ring(
        NY, y, ydev,
        lambda p: wo.at[p, pl.ds(pl.multiple_of(128 * c, 128), 128), :],
        lambda p, h: wo.at[p, pl.ds(pl.multiple_of(128 * c + 64 * h, 64), 64), :],
        pairs(s_ywo, r_ywo), log,
    )
    ring_h = Ring(
        NY, y, ydev,
        lambda p: hid.at[p],
        lambda p, h: hid.at[p, :, pl.ds(1024 * h, 1024)],
        pairs(s_yh, r_yh), log,
        travel=((0, 0), (1, 1), (0, 1), (1, 0)),
    )

    def x_ring(k):
        p = zk(k)
        return Ring(
            NX, x, xdev,
            lambda q: w3.at[:, p, q, c],
            lambda q, h: w3.at[:, p, q, c, pl.ds(16 * h, 16), :],
            [(s_xw.at[k % NZ, d], r_xw.at[k % NZ, d]) for d in (0, 1)], log,
        )

    xr = {k: x_ring(k) for k in (0, -1, 1, -2, 2, -3, 3, 4)}

    def kv_out(k):
        to_partner(kvr.at[zk(k), c], s_dkv.at[k % NZ], r_dkv.at[k % NZ])

    def kv_in(k):
        come(kvr.at[zk(k), 1 - c], s_dkv.at[k % NZ], r_dkv.at[k % NZ])

    def w_out(k):
        to_partner(w3.at[:, zk(k), :, c], s_dw.at[k % NZ], r_dw.at[k % NZ])

    def w_in(k):
        come(w3.at[:, zk(k), :, 1 - c], s_dw.at[k % NZ], r_dw.at[k % NZ])

    def wo_out(k):
        to_partner(ring_wo.blk(ring_wo.at(k)), s_dwo.at[k % NY - 1], r_dwo.at[k % NY - 1])

    def wo_in(k):
        ref = wo.at[ring_wo.at(k), pl.ds(pl.multiple_of(128 - 128 * c, 128), 128), :]
        come(ref, s_dwo.at[k % NY - 1], r_dwo.at[k % NY - 1])

    kvr[z, c, :, rows48(x), :] = kvsend[x]

    cs, sn = table[:, :ROPE], table[:, ROPE : 2 * ROPE]
    q = q_ref[...].astype(F32)
    for h in range(4):
        qr = q[:, 96 * h + HD : 96 * h + 96]
        turned = qr * cs + jnp.concatenate([qr[:, ROPE // 2 :], qr[:, : ROPE // 2]], axis=1) * sn
        full = jnp.concatenate([q[:, 96 * h : 96 * h + HD], turned, jnp.zeros((T, 32), F32)], axis=1)
        qsend[h] = full.astype(BF)
    qin[x] = qsend[x]
    resb[y] = res_ref[rows48(y), :]
    kvt[...] = jnp.ones_like(kvt)
    obuf[...] = jnp.zeros_like(obuf)
    mbuf[...] = jnp.full_like(mbuf, -1e30)

    pl.semaphore_wait(barrier, len(peers))

    for d in (0, 1):
        ring_kv.send(z, d, 0, 0)
    for dx in (1, 3, 2):
        xt = mod4(x + dx)
        go(rcopy(kvsend.at[xt], kvr.at[z, c, :, rows48(x), :], s_kvx.at[dx - 1], r_kvx.at[dx - 1], xdev(xt)))
    ring_w.start()
    for dx in (1, 3, 2):
        xt = mod4(x + dx)
        go(rcopy(qsend.at[xt], qin.at[x], s_qx.at[dx - 1], r_qx.at[dx - 1], xdev(xt)))
    xr[0].start()

    for dy in (1, 3, 2):
        yt = mod4(y + dy)
        go(rcopy(res_ref.at[rows48(yt), :], resb.at[y], s_res.at[dy - 1], r_res.at[dy - 1], ydev(yt)))
        go(rcopy(gains.at[y], gains.at[y], s_g.at[dy - 1], r_g.at[dy - 1], ydev(yt)))
    ring_wo.start()

    for dx in (1, 3, 2):
        come(kvr.at[z, c, :, rows48(mod4(x - dx)), :], s_kvx.at[dx - 1], r_kvx.at[dx - 1])
        for d in (0, 1):
            ring_kv.send(z, d, 0, dx)
    kv_out(0)
    ring_w.step(1)

    for dx in (1, 3, 2):
        come(qin.at[mod4(x - dx)], s_qx.at[dx - 1], r_qx.at[dx - 1])
    qt[...] = jnp.transpose(qin[...].reshape(NQ, 128))

    def attend(p):
        for cc in range(2):
            kr = kvr[p, cc, 4]
            for i in range(4):
                lo = (cc * 4 + i) * T
                kp[lo : lo + T] = jnp.concatenate(
                    [kvr[p, cc, i][:, :HD], kr[:, ROPE * i : ROPE * i + ROPE], jnp.zeros((T, ROPE), BF)], axis=1
                )
            kvt[cc, HD:128] = jnp.transpose(kvr[p, cc, 0:4].reshape(NQ, 128))[HD:128]

        def scores(qb, j):
            s = jnp.dot(kp[T * j : T * j + T], qt[:, QB * qb : QB * qb + QB], preferred_element_type=F32)
            sbuf[qb % 2, T * j : T * j + T] = s
            return jnp.max(s.reshape(T // 8, 8, QB), axis=0)

        maxima = [scores(0, j) for j in range(8)]
        for qb in range(3):
            qs = slice(QB * qb, QB * qb + QB)
            b = qb % 2
            top = maxima[0]
            for other in maxima[1:]:
                top = jnp.maximum(top, other)
            m_old = mbuf[0:1, qs]
            m_new = jnp.maximum(m_old, jnp.max(top, axis=0, keepdims=True))
            mbuf[0:1, qs] = m_new
            factor = jnp.exp2((m_old - m_new) * SCALE)
            shift = m_new * SCALE
            maxima = []
            acc = None
            for j in range(8):
                if qb < 2:
                    maxima.append(scores(qb + 1, j))
                pbuf[b, T * j : T * j + T] = jnp.exp2(sbuf[b, T * j : T * j + T] * SCALE - shift).astype(BF)
                if j % 4 == 3:
                    cc = j // 4
                    got = jnp.dot(kvt[cc], pbuf[b, cc * NQ : cc * NQ + NQ], preferred_element_type=F32)
                    acc = got if acc is None else acc + got
            obuf[:, qs] = obuf[:, qs] * factor + acc

    xr[-1].start()
    xr[1].start()
    kv_in(0)
    attend(z)
    ring_kv.step(1)
    kv_out(-1)
    kv_out(1)
    xr[0].step(1)
    kv_in(-1)
    attend(zk(-1))
    ring_w.take(2)
    xr[-2].start()
    xr[2].start()
    kv_in(1)
    attend(zk(1))
    ring_kv.step(2)
    kv_out(-2)
    kv_out(2)
    ring_w.pass_on(2)
    xr[0].step(2)
    w_out(0)
    xr[-1].step(1)
    xr[1].step(1)
    kv_in(-2)
    attend(zk(-2))
    kv_in(2)
    attend(zk(2))
    ring_kv.step(3)
    kv_out(-3)
    kv_out(3)
    xr[-1].step(2)
    w_out(-1)
    xr[1].step(2)
    w_out(1)
    xr[-2].step(1)
    xr[2].step(1)
    ring_wo.step(1)
    wo_out(-1)
    wo_out(1)
    kv_in(-3)
    attend(zk(-3))
    ring_kv.step(4)
    kv_out(4)
    ring_w.step(3)
    xr[-3].start()
    xr[3].start()
    ring_wo.step(2)
    wo_out(2)
    kv_in(3)
    attend(zk(3))
    xr[-2].step(2)
    w_out(-2)
    xr[2].step(2)
    w_out(2)
    kv_in(4)
    attend(zk(4))
    ring_w.take(4)
    xr[4].start()

    par = lax.rem(x, 2).astype(F32)
    on = obuf[HD:128] / obuf[0:1]
    full = jnp.concatenate([on * (1.0 - par), on * par], axis=0)
    osend[...] = jnp.transpose(full).astype(BF).reshape(4, T, 128)
    others = [(dx, dy) for dx in range(4) for dy in range(4) if dx or dy]
    for dx, dy in sorted(others, key=lambda o: -(min(o[0], 4 - o[0]) + min(o[1], 4 - o[1]))):
        xt, yt = mod4(x + dx), mod4(y + dy)
        n = dx * 4 + dy - 1
        go(rcopy(osend.at[xt, rows48(yt), :], hb.at[4 * y + x], s_o.at[n], r_o.at[n], dev(z, xt, c, yt)))
    hb[4 * y + x] = osend[x, rows48(y), :]
    for dy in (1, 3, 2):
        yf = mod4(y - dy)
        come(resb.at[yf], s_res.at[dy - 1], r_res.at[dy - 1])
        come(gains.at[yf], s_g.at[dy - 1], r_g.at[dy - 1])
    for kk in (-1, 1, 2):
        wo_in(kk)
    for dx, dy in others:
        n = dx * 4 + dy - 1
        come(hb.at[4 * mod4(y - dy) + mod4(x - dx)], s_o.at[n], r_o.at[n])

    attn = None
    for g in range(4):
        heads = [hb[4 * g + 2 * j] + hb[4 * g + 2 * j + 1] for j in range(2)]
        term = jnp.dot(jnp.concatenate(heads, axis=1), wo[g], preferred_element_type=F32)
        term = term.astype(BF).astype(F32)
        attn = term if attn is None else attn + term
    res = jnp.concatenate([resb[g] for g in range(4)], axis=1).astype(F32)
    rows = ALPHA * res + attn
    mean = jnp.sum(rows, axis=1, keepdims=True) * (1.0 / D)
    var = jnp.sum(rows * rows, axis=1, keepdims=True) * (1.0 / D) - mean * mean
    gain = jnp.concatenate([gains[g, 0] for g in range(4)], axis=1)
    hid[y] = ((rows - mean) * lax.rsqrt(var + EPS) * gain).astype(BF)

    ring_h.start()
    xr[-3].step(1)
    xr[3].step(1)
    xr[4].step(1)
    xr[-3].step(2)
    w_out(-3)
    xr[3].step(2)
    w_out(3)
    ring_h.step(1)
    xr[4].step(2)
    w_out(4)
    for kk in (0, -1, 1, -2, 2, -3, 3, 4):
        w_in(kk)

    def gate_up(blocks, lo):
        rows = blocks[0] if len(blocks) == 1 else jnp.concatenate(blocks, axis=0)
        n = rows.shape[0]

        def one(j, carry):
            cols = pl.ds(pl.multiple_of(j * QB, QB), QB)
            gate = jnp.dot(rows, w3[0, :, :, :, :, cols].reshape(D, QB), preferred_element_type=F32)
            up = jnp.dot(rows, w3[1, :, :, :, :, cols].reshape(D, QB), preferred_element_type=F32)
            mixed[lo : lo + n, cols] = (gate / (1.0 + jnp.exp(-gate)) * up).astype(BF)
            return carry

        lax.fori_loop(0, FC // QB, one, 0)

    dist = (0, -1, 1, 2)

    def down(slot, count):
        units = mixed[TQ * slot : TQ * (slot + count)]
        slots = slice(slot, slot + count)
        for dy in (2, 1, 3, 0):
            yt = mod4(y + dy)
            w = w3[2, pl.ds(2 * yt, 2)].reshape(512, FC)
            got = lax.dot_general(units, w, (((1,), (1,)), ((), ())), preferred_element_type=F32)
            got = got.astype(BF).reshape(count, TQ, 512)
            if dy:
                n = min(slot, 1)
                part[dy - 1, slots] = got
                src = part.at[dy - 1, pl.ds(slot, count)]
                dst = crec.at[dy - 1, pl.ds(slot, count)]
                go(rcopy(src, dst, s_p.at[dy - 1, n], r_p.at[dy - 1, n], ydev(yt)))
            else:
                for s in range(count):
                    acc[mod4(y + dist[slot + s])] = got[s].astype(F32)

    gate_up([hid[y], hid[mod4(y - 1)], hid[mod4(y + 1)]], 0)
    down(0, 3)
    ring_h.step(2)
    gate_up([hid[mod4(y + 2)]], 3 * TQ)
    down(3, 1)
    for n, slots in ((0, (0, 1, 2)), (1, (3,))):
        for dy in (1, 3, 2):
            come(crec.at[dy - 1, pl.ds(slots[0], len(slots))], s_p.at[dy - 1, n], r_p.at[dy - 1, n])
            for s in slots:
                b = mod4(y - dy + dist[s])
                acc[b] = acc[b] + crec[dy - 1, s].astype(F32)
    total = acc[...]
    rows = (ALPHA * hid[:, :, cols512(y)].astype(F32) + HALF * total).reshape(T, 512)
    lane = lax.broadcasted_iota(jnp.int32, (T, 128), 1)
    s1 = jnp.sum(rows, axis=1, keepdims=True)
    s2 = jnp.sum(rows * rows, axis=1, keepdims=True)
    sums = jnp.where(lane == 0, s1, jnp.where(lane == 1, s2, 0.0))
    stat[0] = jnp.transpose(sums)[0:8]
    for dy in (2, 1, 3):
        go(rcopy(stat.at[0], stat.at[dy], s_f.at[dy - 1], r_f.at[dy - 1], ydev(mod4(y + dy))))
    both = stat[0]
    for dy in (1, 3, 2):
        come(stat.at[dy], s_f.at[dy - 1], r_f.at[dy - 1])
        both = both + stat[dy]
    both = jnp.transpose(jnp.concatenate([both, jnp.zeros((120, T), F32)], axis=0))
    mean = both[:, 0:1] * (1.0 / D)
    var = both[:, 1:2] * (1.0 / D) - mean * mean
    out_ref[...] = ((rows - mean) * lax.rsqrt(var + EPS) * gains[y, 1]).astype(BF)
    for cp in log:
        cp.wait_send()


def local(queries, latents, rope_key, w_key, w_value, w_out, resid, gain_mix, w_gate, w_up, w_down, gain_out):
    start = lax.axis_index("sp") * T
    positions = start + jnp.arange(T, dtype=jnp.int32)
    grid_rows = (positions // GRID_W).astype(F32)
    grid_cols = (positions % GRID_W).astype(F32)
    count = ROPE // 4
    inverse = ROTARY_BASE ** (-jnp.arange(count, dtype=F32) / count)
    angles = jnp.concatenate([inverse[:, None] * grid_rows, inverse[:, None] * grid_cols], axis=0)
    cos, sin = jnp.cos(angles), jnp.sin(angles)
    cs = jnp.concatenate([cos, cos], axis=0)
    sn = jnp.concatenate([-sin, sin], axis=0)
    dma = pltpu.SemaphoreType.DMA
    V = pltpu.VMEM

    def pair(*shape):
        return [dma(shape), dma(shape)]

    sems = []
    for shape in (
        (3,), (3,), (3,), (3,),
        (2, 4, 4), (8,), (2, 4), (8, 2, 2), (8,),
        (2, 2), (3,),
        (15,), (2, 2, 2), (3, 2), (3,),
    ):
        sems += pair(*shape)
    scratch = [
        V((4, 5, TQ, 128), BF),
        V((4, T, 128), BF),
        V((NZ, 2, 5, T, 128), BF),
        V((4, T, 128), BF),
        V((128, NQ), BF),
        V((8 * T, 128), BF),
        V((2, 128, NQ), BF),
        V((2, 8 * T, QB), F32),
        V((2, 8 * T, QB), BF),
        V((128, NQ), F32),
        V((8, NQ), F32),
        V((4, T, 128), BF),
        V((16, TQ, 128), BF),
        V((NY, 256, D), BF),
        V((NY, TQ, 512), BF),
        V((NY, 2, 1, 512), F32),
        V((3, NZ, NX, 2, 32, FC), BF),
        V((NY, TQ, D), BF),
        V((T, FC), BF),
        V((3, NY, TQ, 512), BF),
        V((3, NY, TQ, 512), BF),
        V((NY, TQ, 512), F32),
        V((NY, 8, T), F32),
    ]
    vm = pl.BlockSpec(memory_space=pltpu.VMEM)
    return pl.pallas_call(
        kernel,
        out_shape=jax.ShapeDtypeStruct((T, 512), BF),
        in_specs=[vm] * 14,
        out_specs=vm,
        scratch_shapes=scratch + sems,
        compiler_params=pltpu.CompilerParams(
            collective_id=0, has_side_effects=True, vmem_limit_bytes=60 * 1024 * 1024
        ),
    )(
        queries, latents, rope_key.T, w_key, w_value, w_out, resid, gain_mix.reshape(1, 512),
        w_gate, w_up, w_down.T, gain_out.reshape(1, 512), cs, sn,
    )


def solution(mesh):
    placed = (
        P("sp", "tp"), P("sp", None), P("sp", None), P(None, "tp"), P(None, "tp"), P("tp", None),
        P("sp", "tp"), P("tp"), P("sp", "tp"), P("sp", "tp"), P("tp", "sp"), P("tp"),
    )
    return jax.shard_map(local, mesh=mesh, in_specs=placed, out_specs=P("sp", "tp"), check_vma=False)
```

```python
import jax
import jax.numpy as jnp
from jax import lax
from jax.experimental import pallas as pl
from jax.experimental.pallas import tpu as pltpu
from jax.sharding import PartitionSpec as P

MESH = pl.DeviceIdType.MESH
F32 = jnp.float32
BF = jnp.bfloat16

HD = 64
ROPE = 32
GRID_W = 64
ROTARY_BASE = 10000.0
EPS = 1e-06
ALPHA = 8.0**0.25
HALF = 0.5
NZ, NX, NY = 8, 4, 4
T = 192
TQ = 48
NQ = 768
QB = 256
D = 2048
FC = 768
SCALE = (1.4426950408889634) * (96.0**-0.5)


class Ring:
    WHOLE = ((0, None), (1, None))
    HALVES = ((0, 0), (1, 1))

    def __init__(self, n, pos, dev, blk, half, sems, log, travel=WHOLE, last=HALVES):
        self.n, self.pos, self.dev, self.travel, self.last = n, pos, dev, travel, last
        self.blk, self.half, self.sems, self.log = blk, half, sems, log
        self.pieces = travel is not self.WHOLE

    def at(self, k):
        return lax.rem(self.pos + (k + 2 * self.n), self.n)

    def copy(self, p, d, t, h):
        ss, rs = self.sems[d]
        ref = self.blk(p) if h is None else self.half(p, h)
        at = (t, h) if self.pieces else (t,)
        return pltpu.make_async_remote_copy(
            src_ref=ref,
            dst_ref=ref,
            send_sem=ss.at[at],
            recv_sem=rs.at[at],
            device_id=self.dev(self.at(1 if d == 0 else -1)),
            device_id_type=MESH,
        )

    def parts(self, t):
        return self.last if t == self.n // 2 - 1 else self.travel

    def send(self, p, d, t, h):
        cp = self.copy(p, d, t, h)
        cp.start()
        self.log.append(cp)

    def start(self):
        for d, h in self.parts(0):
            self.send(self.pos, d, 0, h)

    def arrived(self, d, t):
        return self.at(-t if d == 0 else t)

    def take(self, t):
        for d, h in self.parts(t - 1):
            self.copy(self.arrived(d, t), d, t - 1, h).wait_recv()

    def pass_on(self, t):
        for d, h in self.parts(t):
            self.send(self.arrived(d, t), d, t, h)

    def step(self, t):
        for d, h in self.parts(t - 1):
            p = self.arrived(d, t)
            self.copy(p, d, t - 1, h).wait_recv()
            if self.pieces and t < self.n // 2 and (d, h) in self.parts(t):
                self.send(p, d, t, h)
        if not self.pieces and t < self.n // 2:
            self.pass_on(t)


def kernel(
    q_ref, lat_ref, rk_ref, wk_ref, wv_ref, wo_ref, res_ref, gm_ref, wg_ref, wu_ref, wd_ref, go_ref, cs_ref, sn_ref,
    out_ref,
    kvsend, qsend, kvr, qin, qt, kp, kvt, sbuf, pbuf, obuf, mbuf, osend, hb, wo, resb, gains,
    w3, hid, gacc, mixed, part, crec, acc, stat,
    s_kvx, r_kvx, s_qx, r_qx, s_res, r_res, s_g, r_g,
    s_zkv, r_zkv, s_dkv, r_dkv, s_zw, r_zw, s_xw, r_xw, s_dw, r_dw, s_ywo, r_ywo, s_dwo, r_dwo,
    s_o, r_o, s_yh, r_yh, s_p, r_p, s_f, r_f,
):
    sp = lax.axis_index("sp")
    y = lax.axis_index("tp")
    c = lax.rem(sp, 2)
    x = lax.rem(sp // 2, NX)
    z = sp // (2 * NX)
    log = []

    def dev(zz, xx, cc, yy):
        return ((zz * NX + xx) * 2 + cc, yy)

    def mod4(v):
        return lax.rem(v + 8, 4)

    def zk(k):
        return lax.rem(z + k + NZ, NZ)

    partner = dev(z, x, 1 - c, y)

    def rcopy(src, dst, ss, rs, to):
        return pltpu.make_async_remote_copy(
            src_ref=src, dst_ref=dst, send_sem=ss, recv_sem=rs, device_id=to, device_id_type=MESH
        )

    def go(cp):
        cp.start()
        log.append(cp)

    def come(ref, ss, rs):
        rcopy(ref, ref, ss, rs, partner).wait_recv()

    def to_partner(ref, ss, rs):
        go(rcopy(ref, ref, ss, rs, partner))

    def rows48(i):
        return pl.ds(pl.multiple_of(TQ * i, 16), TQ)

    def cols512(i):
        return pl.ds(pl.multiple_of(512 * i, 512), 512)

    barrier = pltpu.get_barrier_semaphore()
    peers = [dev(z, mod4(x + dx), c, mod4(y + dy)) for dx in range(4) for dy in range(4) if dx or dy]
    peers += [dev(zk(1), x, c, y), dev(zk(-1), x, c, y), partner]
    for peer in peers:
        pl.semaphore_signal(barrier, inc=1, device_id=peer, device_id_type=MESH)

    w3[0, z, x, c] = wg_ref[...]
    w3[1, z, x, c] = wu_ref[...]
    w3[2, z, x, c] = wd_ref[...]
    wo[y] = wo_ref[...]
    gains[y, 0] = gm_ref[...]
    gains[y, 1] = go_ref[...]
    lat = lat_ref[...]
    k = jnp.dot(lat, wk_ref[...], preferred_element_type=F32)
    v = jnp.dot(lat, wv_ref[...], preferred_element_type=F32)
    cst, snt, rkt = cs_ref[...], sn_ref[...], rk_ref[...].astype(F32)
    swapped = jnp.concatenate([rkt[ROPE // 2 :], rkt[: ROPE // 2]], axis=0)
    krt = rkt * cst + swapped * snt
    table = jnp.transpose(jnp.concatenate([cst, snt, krt, krt], axis=0))
    kr = table[:, 2 * ROPE : 3 * ROPE]
    krp = jnp.concatenate([kr[TQ * i : TQ * i + TQ] for i in range(4)], axis=1).astype(BF)
    for h in range(4):
        kv = jnp.concatenate([k[:, HD * h : HD * h + HD], v[:, HD * h : HD * h + HD]], axis=1).astype(BF)
        for i in range(4):
            kvsend[h, i] = kv[TQ * i : TQ * i + TQ]
        kvsend[h, 4] = krp

    zdev = lambda p: dev(p, x, c, y)
    xdev = lambda p: dev(z, p, c, y)
    ydev = lambda p: dev(z, x, c, p)

    def pairs(ss, rs):
        return [(ss.at[d], rs.at[d]) for d in (0, 1)]

    ring_kv = Ring(
        NZ, z, zdev,
        lambda p: kvr.at[p, c],
        lambda p, h: kvr.at[p, c, :, rows48(mod4(x - h)), :],
        pairs(s_zkv, r_zkv), log,
        travel=tuple((d, h) for h in (0, 1, 3, 2) for d in (0, 1)),
        last=((0, 0), (1, 3), (0, 1), (1, 2)),
    )
    ring_w = Ring(
        NZ, z, zdev,
        lambda p: w3.at[:, p, x, c],
        lambda p, h: w3.at[:, p, x, c, pl.ds(16 * h, 16), :],
        pairs(s_zw, r_zw), log,
    )
    ring_wo = Ring(
        NY, y, ydev,
        lambda p: wo.at[p, pl.ds(pl.multiple_of(128 * c, 128), 128), :],
        lambda p, h: wo.at[p, pl.ds(pl.multiple_of(128 * c + 64 * h, 64), 64), :],
        pairs(s_ywo, r_ywo), log,
    )
    ring_h = Ring(
        NY, y, ydev,
        lambda p: hid.at[p],
        lambda p, h: hid.at[p, :, pl.ds(1024 * h, 1024)],
        pairs(s_yh, r_yh), log,
        travel=((0, 0), (1, 1), (0, 1), (1, 0)),
    )

    def x_ring(k):
        p = zk(k)
        return Ring(
            NX, x, xdev,
            lambda q: w3.at[:, p, q, c],
            lambda q, h: w3.at[:, p, q, c, pl.ds(16 * h, 16), :],
            [(s_xw.at[k % NZ, d], r_xw.at[k % NZ, d]) for d in (0, 1)], log,
        )

    xr = {k: x_ring(k) for k in (0, -1, 1, -2, 2, -3, 3)}

    def last_x(dx, slot):
        ref = w3.at[:, zk(4), slot, c]
        at = (4, (dx - 1) // 2, (dx - 1) % 2)
        return rcopy(ref, ref, s_xw.at[at], r_xw.at[at], xdev(mod4(x + dx)))

    def kv_out(k):
        to_partner(kvr.at[zk(k), c], s_dkv.at[k % NZ], r_dkv.at[k % NZ])

    def kv_in(k):
        come(kvr.at[zk(k), 1 - c], s_dkv.at[k % NZ], r_dkv.at[k % NZ])

    def w_out(k):
        to_partner(w3.at[:, zk(k), :, c], s_dw.at[k % NZ], r_dw.at[k % NZ])

    def w_in(k):
        come(w3.at[:, zk(k), :, 1 - c], s_dw.at[k % NZ], r_dw.at[k % NZ])

    def wo_out(k):
        to_partner(ring_wo.blk(ring_wo.at(k)), s_dwo.at[k % NY - 1], r_dwo.at[k % NY - 1])

    def wo_in(k):
        ref = wo.at[ring_wo.at(k), pl.ds(pl.multiple_of(128 - 128 * c, 128), 128), :]
        come(ref, s_dwo.at[k % NY - 1], r_dwo.at[k % NY - 1])

    kvr[z, c, :, rows48(x), :] = kvsend[x]

    cs, sn = table[:, :ROPE], table[:, ROPE : 2 * ROPE]
    q = q_ref[...].astype(F32)
    for h in range(4):
        qr = q[:, 96 * h + HD : 96 * h + 96]
        turned = qr * cs + jnp.concatenate([qr[:, ROPE // 2 :], qr[:, : ROPE // 2]], axis=1) * sn
        full = jnp.concatenate([q[:, 96 * h : 96 * h + HD], turned, jnp.zeros((T, 32), F32)], axis=1)
        qsend[h] = full.astype(BF)
    qin[x] = qsend[x]
    resb[y] = res_ref[rows48(y), :]
    kvt[...] = jnp.ones_like(kvt)
    obuf[...] = jnp.zeros_like(obuf)
    mbuf[...] = jnp.full_like(mbuf, -1e30)

    pl.semaphore_wait(barrier, len(peers))

    for d in (0, 1):
        ring_kv.send(z, d, 0, 0)
    for dx in (1, 3, 2):
        xt = mod4(x + dx)
        go(rcopy(kvsend.at[xt], kvr.at[z, c, :, rows48(x), :], s_kvx.at[dx - 1], r_kvx.at[dx - 1], xdev(xt)))
    ring_w.start()
    for dx in (1, 3, 2):
        xt = mod4(x + dx)
        go(rcopy(qsend.at[xt], qin.at[x], s_qx.at[dx - 1], r_qx.at[dx - 1], xdev(xt)))
    xr[0].start()

    for dy in (1, 3, 2):
        yt = mod4(y + dy)
        go(rcopy(res_ref.at[rows48(yt), :], resb.at[y], s_res.at[dy - 1], r_res.at[dy - 1], ydev(yt)))
        go(rcopy(gains.at[y], gains.at[y], s_g.at[dy - 1], r_g.at[dy - 1], ydev(yt)))
    ring_wo.start()

    for dx in (1, 3, 2):
        come(kvr.at[z, c, :, rows48(mod4(x - dx)), :], s_kvx.at[dx - 1], r_kvx.at[dx - 1])
        for d in (0, 1):
            ring_kv.send(z, d, 0, dx)
    kv_out(0)
    ring_w.step(1)

    for dx in (1, 3, 2):
        come(qin.at[mod4(x - dx)], s_qx.at[dx - 1], r_qx.at[dx - 1])
    qt[...] = jnp.transpose(qin[...].reshape(NQ, 128))

    def attend(p):
        for cc in range(2):
            kr = kvr[p, cc, 4]
            for i in range(4):
                lo = (cc * 4 + i) * T
                kp[lo : lo + T] = jnp.concatenate(
                    [kvr[p, cc, i][:, :HD], kr[:, ROPE * i : ROPE * i + ROPE], jnp.zeros((T, ROPE), BF)], axis=1
                )
            kvt[cc, HD:128] = jnp.transpose(kvr[p, cc, 0:4].reshape(NQ, 128))[HD:128]

        def scores(qb, j):
            s = jnp.dot(kp[T * j : T * j + T], qt[:, QB * qb : QB * qb + QB], preferred_element_type=F32)
            sbuf[qb % 2, T * j : T * j + T] = s
            return jnp.max(s.reshape(T // 8, 8, QB), axis=0)

        maxima = [scores(0, j) for j in range(8)]
        for qb in range(3):
            qs = slice(QB * qb, QB * qb + QB)
            b = qb % 2
            top = maxima[0]
            for other in maxima[1:]:
                top = jnp.maximum(top, other)
            m_old = mbuf[0:1, qs]
            m_new = jnp.maximum(m_old, jnp.max(top, axis=0, keepdims=True))
            mbuf[0:1, qs] = m_new
            factor = jnp.exp2((m_old - m_new) * SCALE)
            shift = m_new * SCALE
            maxima = []
            acc = None
            for j in range(8):
                if qb < 2:
                    maxima.append(scores(qb + 1, j))
                pbuf[b, T * j : T * j + T] = jnp.exp2(sbuf[b, T * j : T * j + T] * SCALE - shift).astype(BF)
                if j % 4 == 3:
                    cc = j // 4
                    got = jnp.dot(kvt[cc], pbuf[b, cc * NQ : cc * NQ + NQ], preferred_element_type=F32)
                    acc = got if acc is None else acc + got
            obuf[:, qs] = obuf[:, qs] * factor + acc

    xr[-1].start()
    xr[1].start()
    kv_in(0)
    attend(z)
    ring_kv.step(1)
    kv_out(-1)
    kv_out(1)
    xr[0].step(1)
    kv_in(-1)
    attend(zk(-1))
    ring_w.take(2)
    xr[-2].start()
    xr[2].start()
    kv_in(1)
    attend(zk(1))
    ring_kv.step(2)
    kv_out(-2)
    kv_out(2)
    ring_w.pass_on(2)
    xr[0].step(2)
    w_out(0)
    xr[-1].step(1)
    xr[1].step(1)
    kv_in(-2)
    attend(zk(-2))
    kv_in(2)
    attend(zk(2))
    ring_kv.step(3)
    kv_out(-3)
    kv_out(3)
    xr[-1].step(2)
    w_out(-1)
    xr[1].step(2)
    w_out(1)
    xr[-2].step(1)
    xr[2].step(1)
    ring_wo.step(1)
    wo_out(-1)
    wo_out(1)
    kv_in(-3)
    attend(zk(-3))
    ring_kv.step(4)
    kv_out(4)
    ring_w.step(3)
    xr[-3].start()
    xr[3].start()
    ring_wo.step(2)
    wo_out(2)
    kv_in(3)
    attend(zk(3))
    xr[-2].step(2)
    w_out(-2)
    xr[2].step(2)
    w_out(2)
    kv_in(4)
    attend(zk(4))
    ring_w.take(4)
    for dx in (2, 1, 3):
        go(last_x(dx, x))

    par = lax.rem(x, 2).astype(F32)
    on = obuf[HD:128] / obuf[0:1]
    full = jnp.concatenate([on * (1.0 - par), on * par], axis=0)
    osend[...] = jnp.transpose(full).astype(BF).reshape(4, T, 128)
    others = [(dx, dy) for dx in range(4) for dy in range(4) if dx or dy]
    for dx, dy in sorted(others, key=lambda o: -(min(o[0], 4 - o[0]) + min(o[1], 4 - o[1]))):
        xt, yt = mod4(x + dx), mod4(y + dy)
        n = dx * 4 + dy - 1
        go(rcopy(osend.at[xt, rows48(yt), :], hb.at[4 * y + x], s_o.at[n], r_o.at[n], dev(z, xt, c, yt)))
    hb[4 * y + x] = osend[x, rows48(y), :]
    for dy in (1, 3, 2):
        yf = mod4(y - dy)
        come(resb.at[yf], s_res.at[dy - 1], r_res.at[dy - 1])
        come(gains.at[yf], s_g.at[dy - 1], r_g.at[dy - 1])
    for kk in (-1, 1, 2):
        wo_in(kk)
    for dx, dy in others:
        n = dx * 4 + dy - 1
        come(hb.at[4 * mod4(y - dy) + mod4(x - dx)], s_o.at[n], r_o.at[n])
    xr[-3].step(1)
    xr[3].step(1)

    attn = None
    for g in range(4):
        heads = [hb[4 * g + 2 * j] + hb[4 * g + 2 * j + 1] for j in range(2)]
        term = jnp.dot(jnp.concatenate(heads, axis=1), wo[g], preferred_element_type=F32)
        term = term.astype(BF).astype(F32)
        attn = term if attn is None else attn + term
    res = jnp.concatenate([resb[g] for g in range(4)], axis=1).astype(F32)
    rows = ALPHA * res + attn
    mean = jnp.sum(rows, axis=1, keepdims=True) * (1.0 / D)
    var = jnp.sum(rows * rows, axis=1, keepdims=True) * (1.0 / D) - mean * mean
    gain = jnp.concatenate([gains[g, 0] for g in range(4)], axis=1)
    hid[y] = ((rows - mean) * lax.rsqrt(var + EPS) * gain).astype(BF)

    ring_h.start()
    xr[-3].step(2)
    w_out(-3)
    xr[3].step(2)
    w_out(3)
    ring_h.step(1)

    def gate_up_block(k, first):
        w_in(k)
        cols = pl.ds(pl.multiple_of(256 * zk(k), 256), 256)
        some = jnp.concatenate([hid[b, :, cols] for b in (y, mod4(y - 1), mod4(y + 1))], axis=0)
        for n in (0, 1):
            term = jnp.dot(some, w3[n, zk(k)].reshape(256, FC), preferred_element_type=F32)
            gacc[n] = term if first else gacc[n] + term

    for kk in (0, -1, 1, -2, 2):
        gate_up_block(kk, kk == 0)
    for dx in (1, 3, 2):
        last_x(dx, mod4(x - dx)).wait_recv()
    w_out(4)
    for kk in (-3, 3, 4):
        gate_up_block(kk, False)
    gate = gacc[0]
    mixed[0 : 3 * TQ] = (gate / (1.0 + jnp.exp(-gate)) * gacc[1]).astype(BF)

    def gate_up(blocks, lo):
        rows = blocks[0] if len(blocks) == 1 else jnp.concatenate(blocks, axis=0)
        n = rows.shape[0]

        def one(j, carry):
            cols = pl.ds(pl.multiple_of(j * QB, QB), QB)
            gate = jnp.dot(rows, w3[0, :, :, :, :, cols].reshape(D, QB), preferred_element_type=F32)
            up = jnp.dot(rows, w3[1, :, :, :, :, cols].reshape(D, QB), preferred_element_type=F32)
            mixed[lo : lo + n, cols] = (gate / (1.0 + jnp.exp(-gate)) * up).astype(BF)
            return carry

        lax.fori_loop(0, FC // QB, one, 0)

    dist = (0, -1, 1, 2)

    def down(slot, count):
        units = mixed[TQ * slot : TQ * (slot + count)]
        slots = slice(slot, slot + count)
        for dy in (2, 1, 3, 0):
            yt = mod4(y + dy)
            w = w3[2, pl.ds(2 * yt, 2)].reshape(512, FC)
            got = lax.dot_general(units, w, (((1,), (1,)), ((), ())), preferred_element_type=F32)
            got = got.astype(BF).reshape(count, TQ, 512)
            if dy:
                n = min(slot, 1)
                part[dy - 1, slots] = got
                src = part.at[dy - 1, pl.ds(slot, count)]
                dst = crec.at[dy - 1, pl.ds(slot, count)]
                go(rcopy(src, dst, s_p.at[dy - 1, n], r_p.at[dy - 1, n], ydev(yt)))
            else:
                for s in range(count):
                    acc[mod4(y + dist[slot + s])] = got[s].astype(F32)

    down(0, 3)
    ring_h.step(2)
    gate_up([hid[mod4(y + 2)]], 3 * TQ)
    down(3, 1)
    for n, slots in ((0, (0, 1, 2)), (1, (3,))):
        for dy in (1, 3, 2):
            come(crec.at[dy - 1, pl.ds(slots[0], len(slots))], s_p.at[dy - 1, n], r_p.at[dy - 1, n])
            for s in slots:
                b = mod4(y - dy + dist[s])
                acc[b] = acc[b] + crec[dy - 1, s].astype(F32)
    total = acc[...]
    rows = (ALPHA * hid[:, :, cols512(y)].astype(F32) + HALF * total).reshape(T, 512)
    lane = lax.broadcasted_iota(jnp.int32, (T, 128), 1)
    s1 = jnp.sum(rows, axis=1, keepdims=True)
    s2 = jnp.sum(rows * rows, axis=1, keepdims=True)
    sums = jnp.where(lane == 0, s1, jnp.where(lane == 1, s2, 0.0))
    stat[0] = jnp.transpose(sums)[0:8]
    for dy in (2, 1, 3):
        go(rcopy(stat.at[0], stat.at[dy], s_f.at[dy - 1], r_f.at[dy - 1], ydev(mod4(y + dy))))
    both = stat[0]
    for dy in (1, 3, 2):
        come(stat.at[dy], s_f.at[dy - 1], r_f.at[dy - 1])
        both = both + stat[dy]
    both = jnp.transpose(jnp.concatenate([both, jnp.zeros((120, T), F32)], axis=0))
    mean = both[:, 0:1] * (1.0 / D)
    var = both[:, 1:2] * (1.0 / D) - mean * mean
    out_ref[...] = ((rows - mean) * lax.rsqrt(var + EPS) * gains[y, 1]).astype(BF)
    for cp in log:
        cp.wait_send()


def local(queries, latents, rope_key, w_key, w_value, w_out, resid, gain_mix, w_gate, w_up, w_down, gain_out):
    start = lax.axis_index("sp") * T
    positions = start + jnp.arange(T, dtype=jnp.int32)
    grid_rows = (positions // GRID_W).astype(F32)
    grid_cols = (positions % GRID_W).astype(F32)
    count = ROPE // 4
    inverse = ROTARY_BASE ** (-jnp.arange(count, dtype=F32) / count)
    angles = jnp.concatenate([inverse[:, None] * grid_rows, inverse[:, None] * grid_cols], axis=0)
    cos, sin = jnp.cos(angles), jnp.sin(angles)
    cs = jnp.concatenate([cos, cos], axis=0)
    sn = jnp.concatenate([-sin, sin], axis=0)
    dma = pltpu.SemaphoreType.DMA
    V = pltpu.VMEM

    def pair(*shape):
        return [dma(shape), dma(shape)]

    sems = []
    for shape in (
        (3,), (3,), (3,), (3,),
        (2, 4, 4), (8,), (2, 4), (8, 2, 2), (8,),
        (2, 2), (3,),
        (15,), (2, 2, 2), (3, 2), (3,),
    ):
        sems += pair(*shape)
    scratch = [
        V((4, 5, TQ, 128), BF),
        V((4, T, 128), BF),
        V((NZ, 2, 5, T, 128), BF),
        V((4, T, 128), BF),
        V((128, NQ), BF),
        V((8 * T, 128), BF),
        V((2, 128, NQ), BF),
        V((2, 8 * T, QB), F32),
        V((2, 8 * T, QB), BF),
        V((128, NQ), F32),
        V((8, NQ), F32),
        V((4, T, 128), BF),
        V((16, TQ, 128), BF),
        V((NY, 256, D), BF),
        V((NY, TQ, 512), BF),
        V((NY, 2, 1, 512), F32),
        V((3, NZ, NX, 2, 32, FC), BF),
        V((NY, TQ, D), BF),
        V((2, 3 * TQ, FC), F32),
        V((T, FC), BF),
        V((3, NY, TQ, 512), BF),
        V((3, NY, TQ, 512), BF),
        V((NY, TQ, 512), F32),
        V((NY, 8, T), F32),
    ]
    vm = pl.BlockSpec(memory_space=pltpu.VMEM)
    return pl.pallas_call(
        kernel,
        out_shape=jax.ShapeDtypeStruct((T, 512), BF),
        in_specs=[vm] * 14,
        out_specs=vm,
        scratch_shapes=scratch + sems,
        compiler_params=pltpu.CompilerParams(
            collective_id=0, has_side_effects=True, vmem_limit_bytes=60 * 1024 * 1024
        ),
    )(
        queries, latents, rope_key.T, w_key, w_value, w_out, resid, gain_mix.reshape(1, 512),
        w_gate, w_up, w_down.T, gain_out.reshape(1, 512), cs, sn,
    )


def solution(mesh):
    placed = (
        P("sp", "tp"), P("sp", None), P("sp", None), P(None, "tp"), P(None, "tp"), P("tp", None),
        P("sp", "tp"), P("tp"), P("sp", "tp"), P("sp", "tp"), P("tp", "sp"), P("tp"),
    )
    return jax.shard_map(local, mesh=mesh, in_specs=placed, out_specs=P("sp", "tp"), check_vma=False)
```

```python
import jax
import jax.numpy as jnp
from jax import lax
from jax.experimental import pallas as pl
from jax.experimental.pallas import tpu as pltpu
from jax.sharding import PartitionSpec as P

MESH = pl.DeviceIdType.MESH
F32 = jnp.float32
BF = jnp.bfloat16

HD = 64
ROPE = 32
GRID_W = 64
ROTARY_BASE = 10000.0
EPS = 1e-06
ALPHA = 8.0**0.25
HALF = 0.5
NZ, NX, NY = 8, 4, 4
T = 192
TQ = 48
NQ = 768
QB = 256
D = 2048
FC = 768
SCALE = (1.4426950408889634) * (96.0**-0.5)


class Ring:
    WHOLE = ((0, None), (1, None))
    HALVES = ((0, 0), (1, 1))

    def __init__(self, n, pos, dev, blk, half, sems, log, travel=WHOLE, last=HALVES):
        self.n, self.pos, self.dev, self.travel, self.last = n, pos, dev, travel, last
        self.blk, self.half, self.sems, self.log = blk, half, sems, log
        self.pieces = travel is not self.WHOLE

    def at(self, k):
        return lax.rem(self.pos + (k + 2 * self.n), self.n)

    def copy(self, p, d, t, h):
        ss, rs = self.sems[d]
        ref = self.blk(p) if h is None else self.half(p, h)
        at = (t, h) if self.pieces else (t,)
        return pltpu.make_async_remote_copy(
            src_ref=ref,
            dst_ref=ref,
            send_sem=ss.at[at],
            recv_sem=rs.at[at],
            device_id=self.dev(self.at(1 if d == 0 else -1)),
            device_id_type=MESH,
        )

    def parts(self, t):
        return self.last if t == self.n // 2 - 1 else self.travel

    def send(self, p, d, t, h):
        cp = self.copy(p, d, t, h)
        cp.start()
        self.log.append(cp)

    def start(self):
        for d, h in self.parts(0):
            self.send(self.pos, d, 0, h)

    def arrived(self, d, t):
        return self.at(-t if d == 0 else t)

    def take(self, t):
        for d, h in self.parts(t - 1):
            self.copy(self.arrived(d, t), d, t - 1, h).wait_recv()

    def pass_on(self, t):
        for d, h in self.parts(t):
            self.send(self.arrived(d, t), d, t, h)

    def step(self, t):
        for d, h in self.parts(t - 1):
            p = self.arrived(d, t)
            self.copy(p, d, t - 1, h).wait_recv()
            if self.pieces and t < self.n // 2 and (d, h) in self.parts(t):
                self.send(p, d, t, h)
        if not self.pieces and t < self.n // 2:
            self.pass_on(t)


def kernel(
    q_ref, lat_ref, rk_ref, wk_ref, wv_ref, wo_ref, res_ref, gm_ref, wg_ref, wu_ref, wd_ref, go_ref, cs_ref, sn_ref,
    out_ref,
    kvsend, qsend, kvr, qin, qt, kp, kvt, sbuf, pbuf, obuf, mbuf, osend, hb, wo, resb, gains,
    w3, hid, mixed, part, crec, acc, stat,
    s_kvx, r_kvx, s_qx, r_qx, s_res, r_res, s_g, r_g,
    s_zkv, r_zkv, s_dkv, r_dkv, s_zw, r_zw, s_xw, r_xw, s_dw, r_dw, s_ywo, r_ywo, s_dwo, r_dwo,
    s_o, r_o, s_yh, r_yh, s_p, r_p, s_f, r_f,
):
    sp = lax.axis_index("sp")
    y = lax.axis_index("tp")
    c = lax.rem(sp, 2)
    x = lax.rem(sp // 2, NX)
    z = sp // (2 * NX)
    log = []

    def dev(zz, xx, cc, yy):
        return ((zz * NX + xx) * 2 + cc, yy)

    def mod4(v):
        return lax.rem(v + 8, 4)

    def zk(k):
        return lax.rem(z + k + NZ, NZ)

    partner = dev(z, x, 1 - c, y)

    def rcopy(src, dst, ss, rs, to):
        return pltpu.make_async_remote_copy(
            src_ref=src, dst_ref=dst, send_sem=ss, recv_sem=rs, device_id=to, device_id_type=MESH
        )

    def go(cp):
        cp.start()
        log.append(cp)

    def come(ref, ss, rs):
        rcopy(ref, ref, ss, rs, partner).wait_recv()

    def to_partner(ref, ss, rs):
        go(rcopy(ref, ref, ss, rs, partner))

    def rows48(i):
        return pl.ds(pl.multiple_of(TQ * i, 16), TQ)

    def cols512(i):
        return pl.ds(pl.multiple_of(512 * i, 512), 512)

    barrier = pltpu.get_barrier_semaphore()
    peers = [dev(z, mod4(x + dx), c, mod4(y + dy)) for dx in range(4) for dy in range(4) if dx or dy]
    peers += [dev(zk(1), x, c, y), dev(zk(-1), x, c, y), partner]
    for peer in peers:
        pl.semaphore_signal(barrier, inc=1, device_id=peer, device_id_type=MESH)

    w3[0, z, x, c] = wg_ref[...]
    w3[1, z, x, c] = wu_ref[...]
    w3[2, z, x, c] = wd_ref[...]
    wo[y] = wo_ref[...]
    gains[y, 0] = gm_ref[...]
    gains[y, 1] = go_ref[...]
    lat = lat_ref[...]
    k = jnp.dot(lat, wk_ref[...], preferred_element_type=F32)
    v = jnp.dot(lat, wv_ref[...], preferred_element_type=F32)
    cst, snt, rkt = cs_ref[...], sn_ref[...], rk_ref[...].astype(F32)
    swapped = jnp.concatenate([rkt[ROPE // 2 :], rkt[: ROPE // 2]], axis=0)
    krt = rkt * cst + swapped * snt
    table = jnp.transpose(jnp.concatenate([cst, snt, krt, krt], axis=0))
    kr = table[:, 2 * ROPE : 3 * ROPE]
    krp = jnp.concatenate([kr[TQ * i : TQ * i + TQ] for i in range(4)], axis=1).astype(BF)
    for h in range(4):
        kv = jnp.concatenate([k[:, HD * h : HD * h + HD], v[:, HD * h : HD * h + HD]], axis=1).astype(BF)
        for i in range(4):
            kvsend[h, i] = kv[TQ * i : TQ * i + TQ]
        kvsend[h, 4] = krp

    zdev = lambda p: dev(p, x, c, y)
    xdev = lambda p: dev(z, p, c, y)
    ydev = lambda p: dev(z, x, c, p)

    def pairs(ss, rs):
        return [(ss.at[d], rs.at[d]) for d in (0, 1)]

    ring_kv = Ring(
        NZ, z, zdev,
        lambda p: kvr.at[p, c],
        lambda p, h: kvr.at[p, c, :, rows48(mod4(x - h)), :],
        pairs(s_zkv, r_zkv), log,
        travel=tuple((d, h) for h in (0, 1, 3, 2) for d in (0, 1)),
        last=((0, 0), (1, 3), (0, 1), (1, 2)),
    )
    ring_w = Ring(
        NZ, z, zdev,
        lambda p: w3.at[:, p, x, c],
        lambda p, h: w3.at[:, p, x, c, pl.ds(16 * h, 16), :],
        pairs(s_zw, r_zw), log,
    )
    ring_wo = Ring(
        NY, y, ydev,
        lambda p: wo.at[p, pl.ds(pl.multiple_of(128 * c, 128), 128), :],
        lambda p, h: wo.at[p, pl.ds(pl.multiple_of(128 * c + 64 * h, 64), 64), :],
        pairs(s_ywo, r_ywo), log,
    )
    ring_h = Ring(
        NY, y, ydev,
        lambda p: hid.at[p],
        lambda p, h: hid.at[p, :, pl.ds(1024 * h, 1024)],
        pairs(s_yh, r_yh), log,
        travel=((0, 0), (1, 1), (0, 1), (1, 0)),
    )

    def x_ring(k):
        p = zk(k)
        return Ring(
            NX, x, xdev,
            lambda q: w3.at[:, p, q, c],
            lambda q, h: w3.at[:, p, q, c, pl.ds(16 * h, 16), :],
            [(s_xw.at[k % NZ, d], r_xw.at[k % NZ, d]) for d in (0, 1)], log,
        )

    xr = {k: x_ring(k) for k in (0, -1, 1, -2, 2, -3, 3, 4)}

    def kv_out(k):
        to_partner(kvr.at[zk(k), c], s_dkv.at[k % NZ], r_dkv.at[k % NZ])

    def kv_in(k):
        come(kvr.at[zk(k), 1 - c], s_dkv.at[k % NZ], r_dkv.at[k % NZ])

    def w_out(k):
        to_partner(w3.at[:, zk(k), :, c], s_dw.at[k % NZ], r_dw.at[k % NZ])

    def w_in(k):
        come(w3.at[:, zk(k), :, 1 - c], s_dw.at[k % NZ], r_dw.at[k % NZ])

    def wo_out(k):
        to_partner(ring_wo.blk(ring_wo.at(k)), s_dwo.at[k % NY - 1], r_dwo.at[k % NY - 1])

    def wo_in(k):
        ref = wo.at[ring_wo.at(k), pl.ds(pl.multiple_of(128 - 128 * c, 128), 128), :]
        come(ref, s_dwo.at[k % NY - 1], r_dwo.at[k % NY - 1])

    kvr[z, c, :, rows48(x), :] = kvsend[x]

    cs, sn = table[:, :ROPE], table[:, ROPE : 2 * ROPE]
    q = q_ref[...].astype(F32)
    for h in range(4):
        qr = q[:, 96 * h + HD : 96 * h + 96]
        turned = qr * cs + jnp.concatenate([qr[:, ROPE // 2 :], qr[:, : ROPE // 2]], axis=1) * sn
        full = jnp.concatenate([q[:, 96 * h : 96 * h + HD], turned, jnp.zeros((T, 32), F32)], axis=1)
        qsend[h] = full.astype(BF)
    qin[x] = qsend[x]
    resb[y] = res_ref[rows48(y), :]
    kvt[...] = jnp.ones_like(kvt)
    obuf[...] = jnp.zeros_like(obuf)
    mbuf[...] = jnp.full_like(mbuf, -1e30)

    pl.semaphore_wait(barrier, len(peers))

    for d in (0, 1):
        ring_kv.send(z, d, 0, 0)
    for dx in (1, 3, 2):
        xt = mod4(x + dx)
        go(rcopy(kvsend.at[xt], kvr.at[z, c, :, rows48(x), :], s_kvx.at[dx - 1], r_kvx.at[dx - 1], xdev(xt)))
    ring_w.start()
    for dx in (1, 3, 2):
        xt = mod4(x + dx)
        go(rcopy(qsend.at[xt], qin.at[x], s_qx.at[dx - 1], r_qx.at[dx - 1], xdev(xt)))
    xr[0].start()

    for dy in (1, 3, 2):
        yt = mod4(y + dy)
        go(rcopy(res_ref.at[rows48(yt), :], resb.at[y], s_res.at[dy - 1], r_res.at[dy - 1], ydev(yt)))
        go(rcopy(gains.at[y], gains.at[y], s_g.at[dy - 1], r_g.at[dy - 1], ydev(yt)))
    ring_wo.start()

    for dx in (1, 3, 2):
        come(kvr.at[z, c, :, rows48(mod4(x - dx)), :], s_kvx.at[dx - 1], r_kvx.at[dx - 1])
        for d in (0, 1):
            ring_kv.send(z, d, 0, dx)
    kv_out(0)
    ring_w.step(1)

    for dx in (1, 3, 2):
        come(qin.at[mod4(x - dx)], s_qx.at[dx - 1], r_qx.at[dx - 1])
    qt[...] = jnp.transpose(qin[...].reshape(NQ, 128))

    def attend(p):
        for cc in range(2):
            kr = kvr[p, cc, 4]
            for i in range(4):
                lo = (cc * 4 + i) * T
                kp[lo : lo + T] = jnp.concatenate(
                    [kvr[p, cc, i][:, :HD], kr[:, ROPE * i : ROPE * i + ROPE], jnp.zeros((T, ROPE), BF)], axis=1
                )
            kvt[cc, HD:128] = jnp.transpose(kvr[p, cc, 0:4].reshape(NQ, 128))[HD:128]

        def scores(qb, j):
            s = jnp.dot(kp[T * j : T * j + T], qt[:, QB * qb : QB * qb + QB], preferred_element_type=F32)
            sbuf[qb % 2, T * j : T * j + T] = s
            return jnp.max(s.reshape(T // 8, 8, QB), axis=0)

        maxima = [scores(0, j) for j in range(8)]
        for qb in range(3):
            qs = slice(QB * qb, QB * qb + QB)
            b = qb % 2
            top = maxima[0]
            for other in maxima[1:]:
                top = jnp.maximum(top, other)
            m_old = mbuf[0:1, qs]
            m_new = jnp.maximum(m_old, jnp.max(top, axis=0, keepdims=True))
            mbuf[0:1, qs] = m_new
            factor = jnp.exp2((m_old - m_new) * SCALE)
            shift = m_new * SCALE
            maxima = []
            acc = None
            for j in range(8):
                if qb < 2:
                    maxima.append(scores(qb + 1, j))
                pbuf[b, T * j : T * j + T] = jnp.exp2(sbuf[b, T * j : T * j + T] * SCALE - shift).astype(BF)
                if j % 4 == 3:
                    cc = j // 4
                    got = jnp.dot(kvt[cc], pbuf[b, cc * NQ : cc * NQ + NQ], preferred_element_type=F32)
                    acc = got if acc is None else acc + got
            obuf[:, qs] = obuf[:, qs] * factor + acc

    xr[-1].start()
    xr[1].start()
    kv_in(0)
    attend(z)
    ring_kv.step(1)
    kv_out(-1)
    kv_out(1)
    xr[0].step(1)
    kv_in(-1)
    attend(zk(-1))
    ring_w.take(2)
    xr[-2].start()
    xr[2].start()
    kv_in(1)
    attend(zk(1))
    ring_kv.step(2)
    kv_out(-2)
    kv_out(2)
    ring_w.pass_on(2)
    xr[0].step(2)
    w_out(0)
    xr[-1].step(1)
    xr[1].step(1)
    kv_in(-2)
    attend(zk(-2))
    kv_in(2)
    attend(zk(2))
    ring_kv.step(3)
    kv_out(-3)
    kv_out(3)
    xr[-1].step(2)
    w_out(-1)
    xr[1].step(2)
    w_out(1)
    xr[-2].step(1)
    xr[2].step(1)
    ring_wo.step(1)
    wo_out(-1)
    wo_out(1)
    kv_in(-3)
    attend(zk(-3))
    ring_kv.step(4)
    kv_out(4)
    ring_w.step(3)
    xr[-3].start()
    xr[3].start()
    ring_wo.step(2)
    wo_out(2)
    kv_in(3)
    attend(zk(3))
    xr[-2].step(2)
    w_out(-2)
    xr[2].step(2)
    w_out(2)
    kv_in(4)
    attend(zk(4))
    ring_w.take(4)
    xr[4].start()

    par = lax.rem(x, 2).astype(F32)
    on = obuf[HD:128] / obuf[0:1]
    full = jnp.concatenate([on * (1.0 - par), on * par], axis=0)
    osend[...] = jnp.transpose(full).astype(BF).reshape(4, T, 128)
    others = [(dx, dy) for dx in range(4) for dy in range(4) if dx or dy]
    for dx, dy in sorted(others, key=lambda o: -(min(o[0], 4 - o[0]) + min(o[1], 4 - o[1]))):
        xt, yt = mod4(x + dx), mod4(y + dy)
        n = dx * 4 + dy - 1
        go(rcopy(osend.at[xt, rows48(yt), :], hb.at[4 * y + x], s_o.at[n], r_o.at[n], dev(z, xt, c, yt)))
    hb[4 * y + x] = osend[x, rows48(y), :]
    for dy in (1, 3, 2):
        yf = mod4(y - dy)
        come(resb.at[yf], s_res.at[dy - 1], r_res.at[dy - 1])
        come(gains.at[yf], s_g.at[dy - 1], r_g.at[dy - 1])
    for kk in (-1, 1, 2):
        wo_in(kk)
    for dx, dy in others:
        n = dx * 4 + dy - 1
        come(hb.at[4 * mod4(y - dy) + mod4(x - dx)], s_o.at[n], r_o.at[n])
    xr[-3].step(1)
    xr[3].step(1)

    attn = None
    for g in range(4):
        heads = [hb[4 * g + 2 * j] + hb[4 * g + 2 * j + 1] for j in range(2)]
        term = jnp.dot(jnp.concatenate(heads, axis=1), wo[g], preferred_element_type=F32)
        term = term.astype(BF).astype(F32)
        attn = term if attn is None else attn + term
    res = jnp.concatenate([resb[g] for g in range(4)], axis=1).astype(F32)
    rows = ALPHA * res + attn
    mean = jnp.sum(rows, axis=1, keepdims=True) * (1.0 / D)
    var = jnp.sum(rows * rows, axis=1, keepdims=True) * (1.0 / D) - mean * mean
    gain = jnp.concatenate([gains[g, 0] for g in range(4)], axis=1)
    hid[y] = ((rows - mean) * lax.rsqrt(var + EPS) * gain).astype(BF)

    ring_h.start()
    xr[4].step(1)
    xr[-3].step(2)
    w_out(-3)
    xr[3].step(2)
    w_out(3)
    ring_h.step(1)
    xr[4].step(2)
    w_out(4)
    for kk in (0, -1, 1, -2, 2, -3, 3, 4):
        w_in(kk)

    def gate_up(blocks, lo):
        rows = blocks[0] if len(blocks) == 1 else jnp.concatenate(blocks, axis=0)
        n = rows.shape[0]

        def one(j, carry):
            cols = pl.ds(pl.multiple_of(j * QB, QB), QB)
            gate = jnp.dot(rows, w3[0, :, :, :, :, cols].reshape(D, QB), preferred_element_type=F32)
            up = jnp.dot(rows, w3[1, :, :, :, :, cols].reshape(D, QB), preferred_element_type=F32)
            mixed[lo : lo + n, cols] = (gate / (1.0 + jnp.exp(-gate)) * up).astype(BF)
            return carry

        lax.fori_loop(0, FC // QB, one, 0)

    dist = (0, -1, 1, 2)

    def down(slot, count):
        units = mixed[TQ * slot : TQ * (slot + count)]
        slots = slice(slot, slot + count)
        for dy in (2, 1, 3, 0):
            yt = mod4(y + dy)
            w = w3[2, pl.ds(2 * yt, 2)].reshape(512, FC)
            got = lax.dot_general(units, w, (((1,), (1,)), ((), ())), preferred_element_type=F32)
            got = got.astype(BF).reshape(count, TQ, 512)
            if dy:
                n = min(slot, 1)
                part[dy - 1, slots] = got
                src = part.at[dy - 1, pl.ds(slot, count)]
                dst = crec.at[dy - 1, pl.ds(slot, count)]
                go(rcopy(src, dst, s_p.at[dy - 1, n], r_p.at[dy - 1, n], ydev(yt)))
            else:
                for s in range(count):
                    acc[mod4(y + dist[slot + s])] = got[s].astype(F32)

    gate_up([hid[y], hid[mod4(y - 1)], hid[mod4(y + 1)]], 0)
    down(0, 3)
    ring_h.step(2)
    gate_up([hid[mod4(y + 2)]], 3 * TQ)
    down(3, 1)
    for n, slots in ((0, (0, 1, 2)), (1, (3,))):
        for dy in (1, 3, 2):
            come(crec.at[dy - 1, pl.ds(slots[0], len(slots))], s_p.at[dy - 1, n], r_p.at[dy - 1, n])
            for s in slots:
                b = mod4(y - dy + dist[s])
                acc[b] = acc[b] + crec[dy - 1, s].astype(F32)
    total = acc[...]
    rows = (ALPHA * hid[:, :, cols512(y)].astype(F32) + HALF * total).reshape(T, 512)
    lane = lax.broadcasted_iota(jnp.int32, (T, 128), 1)
    s1 = jnp.sum(rows, axis=1, keepdims=True)
    s2 = jnp.sum(rows * rows, axis=1, keepdims=True)
    sums = jnp.where(lane == 0, s1, jnp.where(lane == 1, s2, 0.0))
    stat[0] = jnp.transpose(sums)[0:8]
    for dy in (2, 1, 3):
        go(rcopy(stat.at[0], stat.at[dy], s_f.at[dy - 1], r_f.at[dy - 1], ydev(mod4(y + dy))))
    both = stat[0]
    for dy in (1, 3, 2):
        come(stat.at[dy], s_f.at[dy - 1], r_f.at[dy - 1])
        both = both + stat[dy]
    both = jnp.transpose(jnp.concatenate([both, jnp.zeros((120, T), F32)], axis=0))
    mean = both[:, 0:1] * (1.0 / D)
    var = both[:, 1:2] * (1.0 / D) - mean * mean
    out_ref[...] = ((rows - mean) * lax.rsqrt(var + EPS) * gains[y, 1]).astype(BF)
    for cp in log:
        cp.wait_send()


def local(queries, latents, rope_key, w_key, w_value, w_out, resid, gain_mix, w_gate, w_up, w_down, gain_out):
    start = lax.axis_index("sp") * T
    positions = start + jnp.arange(T, dtype=jnp.int32)
    grid_rows = (positions // GRID_W).astype(F32)
    grid_cols = (positions % GRID_W).astype(F32)
    count = ROPE // 4
    inverse = ROTARY_BASE ** (-jnp.arange(count, dtype=F32) / count)
    angles = jnp.concatenate([inverse[:, None] * grid_rows, inverse[:, None] * grid_cols], axis=0)
    cos, sin = jnp.cos(angles), jnp.sin(angles)
    cs = jnp.concatenate([cos, cos], axis=0)
    sn = jnp.concatenate([-sin, sin], axis=0)
    dma = pltpu.SemaphoreType.DMA
    V = pltpu.VMEM

    def pair(*shape):
        return [dma(shape), dma(shape)]

    sems = []
    for shape in (
        (3,), (3,), (3,), (3,),
        (2, 4, 4), (8,), (2, 4), (8, 2, 2), (8,),
        (2, 2), (3,),
        (15,), (2, 2, 2), (3, 2), (3,),
    ):
        sems += pair(*shape)
    scratch = [
        V((4, 5, TQ, 128), BF),
        V((4, T, 128), BF),
        V((NZ, 2, 5, T, 128), BF),
        V((4, T, 128), BF),
        V((128, NQ), BF),
        V((8 * T, 128), BF),
        V((2, 128, NQ), BF),
        V((2, 8 * T, QB), F32),
        V((2, 8 * T, QB), BF),
        V((128, NQ), F32),
        V((8, NQ), F32),
        V((4, T, 128), BF),
        V((16, TQ, 128), BF),
        V((NY, 256, D), BF),
        V((NY, TQ, 512), BF),
        V((NY, 2, 1, 512), F32),
        V((3, NZ, NX, 2, 32, FC), BF),
        V((NY, TQ, D), BF),
        V((T, FC), BF),
        V((3, NY, TQ, 512), BF),
        V((3, NY, TQ, 512), BF),
        V((NY, TQ, 512), F32),
        V((NY, 8, T), F32),
    ]
    vm = pl.BlockSpec(memory_space=pltpu.VMEM)
    return pl.pallas_call(
        kernel,
        out_shape=jax.ShapeDtypeStruct((T, 512), BF),
        in_specs=[vm] * 14,
        out_specs=vm,
        scratch_shapes=scratch + sems,
        compiler_params=pltpu.CompilerParams(
            collective_id=0, has_side_effects=True, vmem_limit_bytes=60 * 1024 * 1024
        ),
    )(
        queries, latents, rope_key.T, w_key, w_value, w_out, resid, gain_mix.reshape(1, 512),
        w_gate, w_up, w_down.T, gain_out.reshape(1, 512), cs, sn,
    )


def solution(mesh):
    placed = (
        P("sp", "tp"), P("sp", None), P("sp", None), P(None, "tp"), P(None, "tp"), P("tp", None),
        P("sp", "tp"), P("tp"), P("sp", "tp"), P("sp", "tp"), P("tp", "sp"), P("tp"),
    )
    return jax.shard_map(local, mesh=mesh, in_specs=placed, out_specs=P("sp", "tp"), check_vma=False)
```
